512 devices in a mesh: rep: 2 (over z_hi), fs: 32 (over z_lo, y), tp: 8 (over x, core).
Axes of the slice: x: 4, y: 4, z: 16 (z_hi: 2, z_lo: 8; z = z_hi * 8 + z_lo), core: 2. Of those that a mesh axis runs over, the one named last changes fastest.
Arguments:
- x_next: bfloat16 [24576, 2048], P(('rep', 'fs')), may hold values from -6 to 6
- value_next: bfloat16 [24576, 3072], P(('rep', 'fs'), 'tp'), may hold values from -6 to 6
- x_prev: bfloat16 [24576, 2048], P(('rep', 'fs')), may hold values from -16 to 16
- value_prev: bfloat16 [24576, 3072], P(('rep', 'fs'), 'tp'), may hold values from -6 to 6
- cotangent: bfloat16 [24576, 3072], P(('rep', 'fs'), 'tp'), may hold values from -16 to 16
- w_gate: bfloat16 [2048, 3072], P('fs', 'tp'), may hold values from -0.125 to 0.125
- conv_taps: float32 [3, 3072], P(None, 'tp'), may hold values from -3.5 to 3.5
- conv_bias: float32 [3072], P('tp'), may hold values from -3 to 3
- sum_w: float32 [2048, 3072], P('fs', 'tp'), may hold values from -6 to 6
- sum_taps: float32 [3, 3072], P(None, 'tp'), may hold values from -6 to 6
- sum_bias: float32 [3072], P('tp'), may hold values from -6 to 6
Outputs:
- hidden_next: bfloat16 [24576, 3072], P(('rep', 'fs'), 'tp')
- grad_input: bfloat16 [24576, 2048], P(('rep', 'fs'))
- grad_value: bfloat16 [24576, 3072], P(('rep', 'fs'), 'tp')
- new_sum_w: float32 [2048, 3072], P('fs', 'tp')
- new_sum_taps: float32 [3, 3072], P(None, 'tp')
- new_sum_bias: float32 [3072], P('tp')
The draws below stay inside these ranges and needn't reach their ends.
All inputs are finite; a program needn't handle non-finite values.
Results may differ from the reference program's by a relative error of at most 0.015.
Values may be sent and summed in bfloat16 or wider, within the bound.
No kernel may reach another device: no remote copies, remote signals or barrier semaphores. Data moves between devices by JAX's collectives and lax.ppermute only.
A program may use at most 64 MiB of HBM per device.

```python
import jax
import jax.numpy as jnp
from jax import lax

D = 2048
F = 3072
TAPS = 3
SEQ_LEN = 128
TOKENS = 24576
N_TP = 8


def raised(entries, own_key, source, target, shards_of, factor):
    def block_of(axis_at):
        return (jnp.arange(entries.shape[axis_at]) // (entries.shape[axis_at] // shards_of)).reshape((-1,) + (1,) * (entries.ndim - 1 - axis_at))

    first = jax.random.permutation(own_key, shards_of)[block_of(target)]
    other_side = (block_of(target) + shards_of // 2) % shards_of
    return jnp.where((block_of(source) == first) | (block_of(source) == other_side), factor * entries, entries)


def shard_levels(rng, shape, shards, low, top_value):
    def one(dim, parts):
        steps = jax.random.uniform(jax.random.fold_in(jax.random.fold_in(rng, 6), dim), (parts,), jnp.float32, low / len(shards), top_value / len(shards))
        return jnp.repeat(jnp.exp(steps), shape[dim] // parts).reshape((-1,) + (1,) * (len(shape) - dim - 1))

    factor_of = one(*shards[0])
    for cut in shards[1:]:
        factor_of = factor_of * one(*cut)
    return factor_of


def noise(own_key, extent, spread, reach, pieces=(), held_as=jnp.bfloat16):
    drawn = jax.random.normal(own_key, extent, jnp.float32) * spread
    if len(pieces) > 0:
        drawn = shard_levels(own_key, extent, pieces, -0.22, 0.18) * drawn
    return jnp.clip(drawn, min=-reach, max=reach).astype(held_as)


def noise_with(key, dims, width, limit, split, heavy, kind=jnp.bfloat16):
    values = width * jax.random.normal(key, dims, jnp.float32)
    if split:
        values = values * shard_levels(key, dims, split, -0.22, 0.18)
    return jnp.clip(raised(values, jax.random.fold_in(key, 3), *heavy), -limit, limit).astype(kind)


def setup_inputs(seed: int = 0) -> dict:
    splits = jax.random.split(jax.random.key(seed), 12)
    x_next = noise(splits[0], (TOKENS, D), 1.0, 6.0, ((0, 64),))
    value_next = noise(splits[1], (TOKENS, F), 1.0, 6.0, ((0, 64), (1, 8)))
    x_prev = noise_with(splits[2], (TOKENS, D), 1.0, 16.0, ((0, 64),), (0, 1, 64, 4.0))
    value_prev = noise(splits[3], (TOKENS, F), 1.0, 6.0, ((0, 64), (1, 8)))
    cotangent = noise_with(splits[4], (TOKENS, F), 1.0, 16.0, ((0, 64), (1, 8)), (0, 1, 64, 4.0))
    w_gate = noise(splits[5], (D, F), D ** -0.5, 0.125, ((0, 32), (1, 8)))
    conv_taps = noise(splits[6], (TAPS, F), TAPS ** -0.5, 3.5, ((1, 8),), jnp.float32)
    conv_bias = noise(splits[7], (F,), 0.5, 3.0, ((0, 8),), jnp.float32)
    sum_w = noise(splits[8], (D, F), 1.0, 6.0, ((0, 32), (1, 8)), jnp.float32)
    sum_taps = noise(splits[9], (TAPS, F), 1.0, 6.0, ((1, 8),), jnp.float32)
    sum_bias = noise(splits[10], (F,), 1.0, 6.0, ((0, 8),), jnp.float32)
    return dict(x_next=x_next, value_next=value_next, x_prev=x_prev, value_prev=value_prev, cotangent=cotangent, w_gate=w_gate, conv_taps=conv_taps, conv_bias=conv_bias, sum_w=sum_w, sum_taps=sum_taps, sum_bias=sum_bias)


def lagged(values, offset, position):
    count_rows = values.shape[0]
    shifted_rows = jnp.concatenate((jnp.zeros((offset, values.shape[1]), values.dtype), values[:count_rows - offset]), axis=0)
    return jnp.where((position >= offset)[:, None], shifted_rows, jnp.zeros_like(shifted_rows))


def leading(values, offset, position):
    shifted_rows = jnp.concatenate((values[offset:], jnp.zeros((offset, values.shape[1]), values.dtype)), axis=0)
    return jnp.where((position < SEQ_LEN - offset)[:, None], shifted_rows, jnp.zeros_like(shifted_rows))


def convolve(up_rows, conv_taps, conv_bias, position):
    values = up_rows.astype(jnp.float32)
    result = jnp.zeros(values.shape, jnp.float32) + conv_bias[None, :]
    for tap_index in range(TAPS):
        result = result + conv_taps[tap_index][None, :] * lagged(values, TAPS - 1 - tap_index, position)
    return result


def reference(x_next, value_next, x_prev, value_prev, cotangent, w_gate, conv_taps, conv_bias, sum_w, sum_taps, sum_bias):
    position = jnp.arange(x_next.shape[0]) % SEQ_LEN
    up_next = jnp.dot(x_next, w_gate, preferred_element_type=jnp.float32).astype(jnp.bfloat16)
    up_prev = jnp.dot(x_prev, w_gate, preferred_element_type=jnp.float32).astype(jnp.bfloat16)
    gate_next = convolve(up_next, conv_taps, conv_bias, position)
    hidden_next = (gate_next * jax.nn.sigmoid(gate_next) * value_next.astype(jnp.float32)).astype(jnp.bfloat16)
    gate_prev = convolve(up_prev, conv_taps, conv_bias, position)
    sigmoid_gate = jax.nn.sigmoid(gate_prev)
    cot_values = cotangent.astype(jnp.float32)
    grad_value = (cot_values * gate_prev * sigmoid_gate).astype(jnp.bfloat16)
    grad_gate = cot_values * value_prev.astype(jnp.float32) * sigmoid_gate * (1.0 + gate_prev * (1.0 - sigmoid_gate))
    grad_up = jnp.zeros(grad_gate.shape, jnp.float32)
    for tap_index in range(TAPS):
        grad_up = grad_up + conv_taps[tap_index][None, :] * leading(grad_gate, TAPS - 1 - tap_index, position)
    grad_up = grad_up.astype(jnp.bfloat16)
    block_width = F // N_TP
    accumulated = jnp.zeros((x_prev.shape[0], w_gate.shape[0]), jnp.float32)
    for index_block in range(N_TP):
        block_part = jnp.dot(grad_up[:, index_block * block_width:(index_block + 1) * block_width],
                             w_gate[:, index_block * block_width:(index_block + 1) * block_width].T,
                             preferred_element_type=jnp.float32)
        accumulated = accumulated + lax.optimization_barrier(block_part.astype(jnp.bfloat16)).astype(jnp.float32)
    grad_input = accumulated.astype(jnp.bfloat16)
    grad_scale = float(x_prev.shape[0]) ** -0.5
    grad_w = jnp.dot(x_prev.T, grad_up, preferred_element_type=jnp.float32) * grad_scale
    up_values = up_prev.astype(jnp.float32)
    grad_taps = jnp.stack([jnp.sum(grad_gate * lagged(up_values, TAPS - 1 - tap_index, position), axis=0) for tap_index in range(TAPS)], axis=0) * grad_scale
    grad_bias = jnp.sum(grad_gate, axis=0) * grad_scale
    return (hidden_next, grad_input, grad_value, sum_w + grad_w, sum_taps + grad_taps, sum_bias + grad_bias)
```

```python
import jax
import jax.numpy as jnp
from jax import lax
from jax.sharding import Mesh
from jax.sharding import PartitionSpec as P

SEQ_LEN = 128
SMALL_ROWS = 8


def copies_to(block, axis, size):
    copies = jnp.broadcast_to(block, (size, *block.shape))
    return lax.all_to_all(copies, axis, 0, 0, tiled=True)


def exchange(blocks, axis):
    return lax.all_to_all(blocks, axis, 0, 0, tiled=True)


def summed(blocks):
    return jnp.sum(blocks.astype(jnp.float32), axis=0)


def lagged(values, offset, position):
    count_rows = values.shape[0]
    shifted_rows = jnp.concatenate(
        (jnp.zeros((offset, values.shape[1]), values.dtype), values[: count_rows - offset]), axis=0
    )
    return jnp.where((position >= offset)[:, None], shifted_rows, jnp.zeros_like(shifted_rows))


def leading(values, offset, position):
    shifted_rows = jnp.concatenate(
        (values[offset:], jnp.zeros((offset, values.shape[1]), values.dtype)), axis=0
    )
    return jnp.where(
        (position < SEQ_LEN - offset)[:, None], shifted_rows, jnp.zeros_like(shifted_rows)
    )


def convolve(up_rows, conv_taps, conv_bias, position):
    values = up_rows.astype(jnp.float32)
    tap_count = conv_taps.shape[0]
    result = jnp.zeros(values.shape, jnp.float32) + conv_bias[None, :]
    for tap_index in range(tap_count):
        result = result + conv_taps[tap_index][None, :] * lagged(
            values, tap_count - 1 - tap_index, position
        )
    return result


def high_and_low(rows):
    high = rows.astype(jnp.bfloat16)
    low = (rows - high.astype(jnp.float32)).astype(jnp.bfloat16)
    return jnp.concatenate([high, low], axis=0)


def with_small(blocks, small):
    rows = jnp.broadcast_to(high_and_low(small), (blocks.shape[0], SMALL_ROWS, small.shape[1]))
    return jnp.concatenate([blocks, rows], axis=1)


def split_small(total):
    rows = total.shape[0] - SMALL_ROWS
    half = SMALL_ROWS // 2
    return total[:rows], total[rows : rows + half] + total[rows + half :]


def per_device(
    x_next,
    value_next,
    x_prev,
    value_prev,
    cotangent,
    w_gate,
    conv_taps,
    conv_bias,
    sum_w,
    sum_taps,
    sum_bias,
):
    row_count, width = x_next.shape
    shard_rows, units = w_gate.shape
    tap_count = conv_taps.shape[0]
    position = jnp.arange(row_count) % SEQ_LEN
    n_zh, n_zm, n_zq, n_y = (lax.axis_size(a) for a in ("zh", "zm", "zq", "y"))
    n_x, n_c = lax.axis_size("x"), lax.axis_size("c")

    pair = copies_to(w_gate, "zm", n_zm)
    quad = copies_to(pair, "zq", n_zq)
    plane = copies_to(quad, "y", n_y)
    gathered = jnp.transpose(plane, (2, 1, 0, 3, 4)).reshape(width, units)

    up_prev = jnp.dot(x_prev, gathered, preferred_element_type=jnp.float32).astype(jnp.bfloat16)
    gate_prev = convolve(up_prev, conv_taps, conv_bias, position)
    sigmoid_gate = jax.nn.sigmoid(gate_prev)
    cot_values = cotangent.astype(jnp.float32)
    grad_value = (cot_values * gate_prev * sigmoid_gate).astype(jnp.bfloat16)
    grad_gate = (
        cot_values
        * value_prev.astype(jnp.float32)
        * sigmoid_gate
        * (1.0 + gate_prev * (1.0 - sigmoid_gate))
    )
    grad_up = jnp.zeros(grad_gate.shape, jnp.float32)
    for tap_index in range(tap_count):
        grad_up = grad_up + conv_taps[tap_index][None, :] * leading(
            grad_gate, tap_count - 1 - tap_index, position
        )
    grad_up = grad_up.astype(jnp.bfloat16)
    token_count = row_count * n_zh * n_zm * n_zq * n_y
    grad_scale = float(token_count) ** (-0.5)
    up_values = up_prev.astype(jnp.float32)
    small = (
        jnp.stack(
            [
                jnp.sum(grad_gate * lagged(up_values, tap_count - 1 - tap_index, position), axis=0)
                for tap_index in range(tap_count)
            ]
            + [jnp.sum(grad_gate, axis=0)],
            axis=0,
        )
        * grad_scale
    )

    grad_w = (
        lax.dot_general(
            x_prev, grad_up, (((0,), (0,)), ((), ())), preferred_element_type=jnp.float32
        )
        * grad_scale
    ).astype(jnp.bfloat16)
    by_y = jnp.transpose(grad_w.reshape(n_zm, n_zq, n_y, shard_rows, units), (2, 1, 0, 3, 4))
    by_y = with_small(by_y.reshape(n_y, n_zq * n_zm * shard_rows, units), small)
    part, small = split_small(summed(exchange(by_y, "y")))
    by_q = part.astype(jnp.bfloat16).reshape(n_zq, n_zm * shard_rows, units)
    part, small = split_small(summed(exchange(with_small(by_q, small), "zq")))
    by_half = part.astype(jnp.bfloat16).reshape(n_zm, shard_rows, units)
    by_half = with_small(by_half, small)
    by_half = jnp.broadcast_to(by_half, (n_zh, *by_half.shape)).reshape(-1, *by_half.shape[1:])
    grad_rows, small = split_small(summed(exchange(by_half, ("zh", "zm"))))

    partial_input = lax.dot_general(
        grad_up, gathered, (((1,), (1,)), ((), ())), preferred_element_type=jnp.float32
    ).astype(jnp.bfloat16)
    half = summed(exchange(partial_input.reshape(n_c, -1, width), "c")).astype(jnp.bfloat16)
    eighth = summed(exchange(half.reshape(n_x, -1, width), "x")).astype(jnp.bfloat16)
    half = copies_to(eighth, "x", n_x).reshape(-1, width)
    grad_input = copies_to(half, "c", n_c).reshape(-1, width)

    up_next = jnp.dot(x_next, gathered, preferred_element_type=jnp.float32).astype(jnp.bfloat16)
    gate_next = convolve(up_next, conv_taps, conv_bias, position)
    hidden_next = (gate_next * jax.nn.sigmoid(gate_next) * value_next.astype(jnp.float32)).astype(
        jnp.bfloat16
    )
    return (
        hidden_next,
        grad_input,
        grad_value,
        sum_w + grad_rows,
        sum_taps + small[:tap_count],
        sum_bias + small[tap_count],
    )


def solution(mesh):
    n_fs, n_tp = mesh.shape["fs"], mesh.shape["tp"]
    n_y, n_zq, n_c = 4, 4, 2
    fine = Mesh(
        mesh.devices.reshape(
            mesh.shape["rep"], n_fs // (n_y * n_zq), n_zq, n_y, n_tp // n_c, n_c
        ),
        ("zh", "zm", "zq", "y", "x", "c"),
    )
    fs, tp = ("zm", "zq", "y"), ("x", "c")
    tokens = ("zh", *fs)
    in_specs = (
        P(tokens, None),
        P(tokens, tp),
        P(tokens, None),
        P(tokens, tp),
        P(tokens, tp),
        P(fs, tp),
        P(None, tp),
        P(tp),
        P(fs, tp),
        P(None, tp),
        P(tp),
    )
    out_specs = (
        P(tokens, tp),
        P(tokens, None),
        P(tokens, tp),
        P(fs, tp),
        P(None, tp),
        P(tp),
    )
    return jax.shard_map(
        per_device, mesh=fine, in_specs=in_specs, out_specs=out_specs, check_vma=False
    )
```

```python
import jax
import jax.numpy as jnp
from jax import lax
from jax.experimental import pallas as pl
from jax.experimental.pallas import tpu as pltpu
from jax.sharding import Mesh
from jax.sharding import PartitionSpec as P

SEQ_LEN = 128
SMALL_ROWS = 8


def copies_to(block, axis, size):
    copies = jnp.broadcast_to(block, (size, *block.shape))
    return lax.all_to_all(copies, axis, 0, 0, tiled=True)


def exchange(blocks, axis):
    return lax.all_to_all(blocks, axis, 0, 0, tiled=True)


def send_on(block, axis, shift):
    size = lax.axis_size(axis)
    return lax.ppermute(block, axis, [(i, (i + shift) % size) for i in range(size)])


def put_in_order(own, other, n_c):
    n_x = own.shape[0]

    def body(own_ref, other_ref, out_ref, sems):
        at_x, at_c = lax.axis_index("x"), lax.axis_index("c")
        moves = []
        for k in range(n_x):
            spot = (at_x + n_x - k) % n_x
            moves.append(
                pltpu.make_async_copy(own_ref.at[k], out_ref.at[at_c * n_x + spot], sems.at[k])
            )
            moves.append(
                pltpu.make_async_copy(
                    other_ref.at[k], out_ref.at[(1 - at_c) * n_x + spot], sems.at[n_x + k]
                )
            )
        for move in moves:
            move.start()
        for move in moves:
            move.wait()

    return pl.pallas_call(
        body,
        out_shape=jax.ShapeDtypeStruct((n_c * n_x, *own.shape[1:]), own.dtype),
        in_specs=[pl.BlockSpec(memory_space=pl.ANY)] * 2,
        out_specs=pl.BlockSpec(memory_space=pl.ANY),
        scratch_shapes=[pltpu.SemaphoreType.DMA((2 * n_x,))],
        cost_estimate=pl.CostEstimate(
            flops=0, bytes_accessed=4 * own.size * own.dtype.itemsize, transcendentals=0
        ),
    )(own, other)


def summed(blocks):
    return jnp.sum(blocks.astype(jnp.float32), axis=0)


def lagged(values, offset, position):
    count_rows = values.shape[0]
    shifted_rows = jnp.concatenate(
        (jnp.zeros((offset, values.shape[1]), values.dtype), values[: count_rows - offset]), axis=0
    )
    return jnp.where((position >= offset)[:, None], shifted_rows, jnp.zeros_like(shifted_rows))


def leading(values, offset, position):
    shifted_rows = jnp.concatenate(
        (values[offset:], jnp.zeros((offset, values.shape[1]), values.dtype)), axis=0
    )
    return jnp.where(
        (position < SEQ_LEN - offset)[:, None], shifted_rows, jnp.zeros_like(shifted_rows)
    )


def convolve(up_rows, conv_taps, conv_bias, position):
    values = up_rows.astype(jnp.float32)
    tap_count = conv_taps.shape[0]
    result = jnp.zeros(values.shape, jnp.float32) + conv_bias[None, :]
    for tap_index in range(tap_count):
        result = result + conv_taps[tap_index][None, :] * lagged(
            values, tap_count - 1 - tap_index, position
        )
    return result


def high_and_low(rows):
    high = rows.astype(jnp.bfloat16)
    low = (rows - high.astype(jnp.float32)).astype(jnp.bfloat16)
    return jnp.concatenate([high, low], axis=0)


def with_small(blocks, small):
    rows = jnp.broadcast_to(high_and_low(small), (blocks.shape[0], SMALL_ROWS, small.shape[1]))
    return jnp.concatenate([blocks, rows], axis=1)


def split_small(total):
    rows = total.shape[0] - SMALL_ROWS
    half = SMALL_ROWS // 2
    return total[:rows], total[rows : rows + half] + total[rows + half :]


def per_device(
    x_next,
    value_next,
    x_prev,
    value_prev,
    cotangent,
    w_gate,
    conv_taps,
    conv_bias,
    sum_w,
    sum_taps,
    sum_bias,
):
    row_count, width = x_next.shape
    shard_rows, units = w_gate.shape
    tap_count = conv_taps.shape[0]
    position = jnp.arange(row_count) % SEQ_LEN
    n_zh, n_zm, n_zq, n_y = (lax.axis_size(a) for a in ("zh", "zm", "zq", "y"))
    n_x, n_c = lax.axis_size("x"), lax.axis_size("c")

    pair = copies_to(w_gate, "zm", n_zm)
    quad = copies_to(pair, "zq", n_zq)
    plane = copies_to(quad, "y", n_y)
    gathered = jnp.transpose(plane, (2, 1, 0, 3, 4)).reshape(width, units)

    up_prev = jnp.dot(x_prev, gathered, preferred_element_type=jnp.float32).astype(jnp.bfloat16)
    gate_prev = convolve(up_prev, conv_taps, conv_bias, position)
    sigmoid_gate = jax.nn.sigmoid(gate_prev)
    cot_values = cotangent.astype(jnp.float32)
    grad_value = (cot_values * gate_prev * sigmoid_gate).astype(jnp.bfloat16)
    grad_gate = (
        cot_values
        * value_prev.astype(jnp.float32)
        * sigmoid_gate
        * (1.0 + gate_prev * (1.0 - sigmoid_gate))
    )
    grad_up = jnp.zeros(grad_gate.shape, jnp.float32)
    for tap_index in range(tap_count):
        grad_up = grad_up + conv_taps[tap_index][None, :] * leading(
            grad_gate, tap_count - 1 - tap_index, position
        )
    grad_up = grad_up.astype(jnp.bfloat16)
    token_count = row_count * n_zh * n_zm * n_zq * n_y
    grad_scale = float(token_count) ** (-0.5)
    up_values = up_prev.astype(jnp.float32)
    small = (
        jnp.stack(
            [
                jnp.sum(grad_gate * lagged(up_values, tap_count - 1 - tap_index, position), axis=0)
                for tap_index in range(tap_count)
            ]
            + [jnp.sum(grad_gate, axis=0)],
            axis=0,
        )
        * grad_scale
    )

    grad_w = (
        lax.dot_general(
            x_prev, grad_up, (((0,), (0,)), ((), ())), preferred_element_type=jnp.float32
        )
        * grad_scale
    ).astype(jnp.bfloat16)
    by_y = jnp.transpose(grad_w.reshape(n_zm, n_zq, n_y, shard_rows, units), (2, 1, 0, 3, 4))
    by_y = with_small(by_y.reshape(n_y, n_zq * n_zm * shard_rows, units), small)
    by_y, grad_up, x_next = lax.optimization_barrier((by_y, grad_up, x_next))
    from_y = exchange(by_y, "y")

    at_x, at_c = lax.axis_index("x"), lax.axis_index("c")
    block_rows = row_count // (n_x * n_c)

    def partial_half(which):
        rows = lax.dynamic_slice_in_dim(grad_up, which * n_x * block_rows, n_x * block_rows, 0)
        turned = lax.dynamic_slice_in_dim(
            jnp.concatenate([rows, rows], axis=0), at_x * block_rows, n_x * block_rows, 0
        )
        return lax.dot_general(
            turned, gathered, (((1,), (1,)), ((), ())), preferred_element_type=jnp.float32
        )

    from_core = send_on(partial_half(1 - at_c).astype(jnp.bfloat16), "c", 1)
    half = (partial_half(at_c) + from_core.astype(jnp.float32)).astype(jnp.bfloat16)
    half = half.reshape(n_x, block_rows, width)
    arrived = [half[0]] + [send_on(half[k], "x", k) for k in range(1, n_x)]
    from_y, *arrived = lax.optimization_barrier((from_y, *arrived))
    eighth = sum(block.astype(jnp.float32) for block in arrived).astype(jnp.bfloat16)
    half = jnp.stack([eighth] + [send_on(eighth, "x", k) for k in range(1, n_x)])
    grad_input = put_in_order(half, send_on(half, "c", 1), n_c).reshape(row_count, width)

    part, small = split_small(summed(from_y))
    by_q = part.astype(jnp.bfloat16).reshape(n_zq, n_zm * shard_rows, units)
    part, small = split_small(summed(exchange(with_small(by_q, small), "zq")))
    by_half = part.astype(jnp.bfloat16).reshape(n_zm, shard_rows, units)
    by_half = with_small(by_half, small)
    by_half = jnp.broadcast_to(by_half, (n_zh, *by_half.shape)).reshape(-1, *by_half.shape[1:])
    grad_rows, small = split_small(summed(exchange(by_half, ("zh", "zm"))))

    up_next = jnp.dot(x_next, gathered, preferred_element_type=jnp.float32).astype(jnp.bfloat16)
    gate_next = convolve(up_next, conv_taps, conv_bias, position)
    hidden_next = (gate_next * jax.nn.sigmoid(gate_next) * value_next.astype(jnp.float32)).astype(
        jnp.bfloat16
    )
    return (
        hidden_next,
        grad_input,
        grad_value,
        sum_w + grad_rows,
        sum_taps + small[:tap_count],
        sum_bias + small[tap_count],
    )


def solution(mesh):
    n_fs, n_tp = mesh.shape["fs"], mesh.shape["tp"]
    n_y, n_zq, n_c = 4, 4, 2
    fine = Mesh(
        mesh.devices.reshape(
            mesh.shape["rep"], n_fs // (n_y * n_zq), n_zq, n_y, n_tp // n_c, n_c
        ),
        ("zh", "zm", "zq", "y", "x", "c"),
    )
    fs, tp = ("zm", "zq", "y"), ("x", "c")
    tokens = ("zh", *fs)
    in_specs = (
        P(tokens, None),
        P(tokens, tp),
        P(tokens, None),
        P(tokens, tp),
        P(tokens, tp),
        P(fs, tp),
        P(None, tp),
        P(tp),
        P(fs, tp),
        P(None, tp),
        P(tp),
    )
    out_specs = (
        P(tokens, tp),
        P(tokens, None),
        P(tokens, tp),
        P(fs, tp),
        P(None, tp),
        P(tp),
    )
    return jax.shard_map(
        per_device, mesh=fine, in_specs=in_specs, out_specs=out_specs, check_vma=False
    )
```

```python
import jax
import jax.numpy as jnp
from jax import lax
from jax.experimental import pallas as pl
from jax.experimental.pallas import tpu as pltpu
from jax.sharding import Mesh
from jax.sharding import PartitionSpec as P


SEQ_LEN = 128
SMALL_ROWS = 8


def copies_to(block, axis, size):
    copies = jnp.broadcast_to(block, (size, *block.shape))
    return lax.all_to_all(copies, axis, 0, 0, tiled=True)


def exchange(blocks, axis):
    return lax.all_to_all(blocks, axis, 0, 0, tiled=True)


def send_on(block, axis, shift):
    size = lax.axis_size(axis)
    return lax.ppermute(block, axis, [(i, (i + shift) % size) for i in range(size)])


def whole(shape):
    return pl.BlockSpec(shape, lambda *_: (0,) * len(shape))


def cost(flops, count, exps=0):
    return pl.CostEstimate(flops=flops, bytes_accessed=count, transcendentals=exps)


def put_in_order(own, other, n_c):
    n_x = len(own)
    rows, width = own[0].shape

    def body(*refs):
        out_ref = refs[-1]
        at_x, at_c = lax.axis_index("x"), lax.axis_index("c")
        for k in range(n_x):
            spot = (at_x + n_x - k) % n_x
            out_ref[at_c * n_x + spot] = refs[k][...]
            out_ref[(1 - at_c) * n_x + spot] = refs[n_x + k][...]

    return pl.pallas_call(
        body,
        out_shape=jax.ShapeDtypeStruct((n_c * n_x, rows, width), own[0].dtype),
        cost_estimate=cost(0, 32 * own[0].size),
        name="put_in_order",
    )(*own, *other)


def later(values, offset):
    rows = lax.broadcasted_iota(jnp.int32, values.shape, 0)
    return values if offset == 0 else jnp.where(
        rows >= offset, pltpu.roll(values, offset, 0), 0.0
    )


def earlier(values, offset):
    count = values.shape[0]
    rows = lax.broadcasted_iota(jnp.int32, values.shape, 0)
    return values if offset == 0 else jnp.where(
        rows < count - offset, pltpu.roll(values, count - offset, 0), 0.0
    )


def gated(up, taps_ref, bias_ref):
    tap_count = taps_ref.shape[0]
    total = bias_ref[...]
    for j in range(tap_count):
        total = total + taps_ref[j : j + 1, :] * later(up, tap_count - 1 - j)
    return total


def previous_branch(x_prev, plane, cotangent, value_prev, conv_taps, conv_bias, n_c):
    row_count, width = x_prev.shape
    n_y, n_zq, n_zm, shard_rows, units = plane.shape
    tap_count = conv_taps.shape[0]
    n_x = lax.axis_size("x")
    half_rows = row_count // n_c
    block_rows = half_rows // n_x
    steps = row_count // SEQ_LEN

    def body(
        x_ref,
        w_ref,
        cot_ref,
        value_ref,
        taps_ref,
        bias_ref,
        gv_ref,
        gu_ref,
        small_ref,
        natural_ref,
        turned_ref,
        send_ref,
    ):
        step = pl.program_id(0)

        @pl.when(step == 0)
        def _():
            small_ref[...] = jnp.zeros_like(small_ref)
            for y in range(n_y):
                for q in range(n_zq):
                    for m in range(n_zm):
                        at = ((m * n_zq + q) * n_y + y) * shard_rows
                        natural_ref[at : at + shard_rows] = w_ref[y, q, m]

        up = jnp.dot(x_ref[...], natural_ref[...], preferred_element_type=jnp.float32)
        up = up.astype(jnp.bfloat16).astype(jnp.float32)
        gate = gated(up, taps_ref, bias_ref)
        sig = jax.nn.sigmoid(gate)
        cot = cot_ref[...].astype(jnp.float32)
        gv_ref[...] = (cot * gate * sig).astype(jnp.bfloat16)
        grad_gate = cot * value_ref[...].astype(jnp.float32) * sig * (1.0 + gate * (1.0 - sig))
        grad_up = jnp.zeros_like(grad_gate)
        for j in range(tap_count):
            grad_up = grad_up + taps_ref[j : j + 1, :] * earlier(grad_gate, tap_count - 1 - j)
        start = pl.multiple_of(step * SEQ_LEN, SEQ_LEN)
        gu_ref[pl.ds(start, SEQ_LEN)] = grad_up.astype(jnp.bfloat16)
        for j in range(tap_count):
            small_ref[j : j + 1, :] += jnp.sum(
                grad_gate * later(up, tap_count - 1 - j), axis=0, keepdims=True
            )
        small_ref[tap_count : tap_count + 1, :] += jnp.sum(grad_gate, axis=0, keepdims=True)

        @pl.when(step == steps - 1)
        def _():
            at_x, at_c = lax.axis_index("x"), lax.axis_index("c")
            for i in range(n_c):
                core = (at_c + 1 + i) % n_c
                for k in range(n_x):
                    row = core * half_rows + ((at_x + k) % n_x) * block_rows
                    turned_ref[i, k * block_rows : (k + 1) * block_rows] = gu_ref[
                        pl.ds(pl.multiple_of(row, block_rows), block_rows)
                    ]
            send_ref[...] = lax.dot_general(
                turned_ref[0],
                natural_ref[...],
                (((1,), (1,)), ((), ())),
                preferred_element_type=jnp.float32,
            ).astype(jnp.bfloat16)

    rows = pl.BlockSpec((SEQ_LEN, units), lambda i: (i, 0))
    half = jax.ShapeDtypeStruct((row_count, units), jnp.bfloat16)
    outs = [
        half,
        half,
        jax.ShapeDtypeStruct((SMALL_ROWS, units), jnp.float32),
        jax.ShapeDtypeStruct((width, units), jnp.bfloat16),
        jax.ShapeDtypeStruct((n_c, half_rows, units), jnp.bfloat16),
        jax.ShapeDtypeStruct((half_rows, width), jnp.bfloat16),
    ]
    return pl.pallas_call(
        body,
        grid=(steps,),
        in_specs=[
            pl.BlockSpec((SEQ_LEN, width), lambda i: (i, 0)),
            whole(plane.shape),
            rows,
            rows,
            whole(conv_taps.shape),
            whole((1, units)),
        ],
        out_specs=[rows] + [whole(o.shape) for o in outs[1:]],
        out_shape=outs,
        cost_estimate=cost(3 * row_count * width * units, 8 * width * units, row_count * units),
        name="previous_branch",
    )(x_prev, plane, cotangent, value_prev, conv_taps, conv_bias.reshape(1, units))


def next_branch(x_next, weights, value_next, conv_taps, conv_bias):
    row_count, width = x_next.shape
    units = weights.shape[1]

    def body(x_ref, w_ref, value_ref, taps_ref, bias_ref, out_ref):
        up = jnp.dot(x_ref[...], w_ref[...], preferred_element_type=jnp.float32)
        gate = gated(up.astype(jnp.bfloat16).astype(jnp.float32), taps_ref, bias_ref)
        hidden = gate * jax.nn.sigmoid(gate) * value_ref[...].astype(jnp.float32)
        out_ref[...] = hidden.astype(jnp.bfloat16)

    rows = pl.BlockSpec((SEQ_LEN, units), lambda i: (i, 0))
    return pl.pallas_call(
        body,
        grid=(row_count // SEQ_LEN,),
        in_specs=[
            pl.BlockSpec((SEQ_LEN, width), lambda i: (i, 0)),
            whole(weights.shape),
            rows,
            whole(conv_taps.shape),
            whole((1, units)),
        ],
        out_specs=rows,
        out_shape=jax.ShapeDtypeStruct((row_count, units), jnp.bfloat16),
        cost_estimate=cost(2 * row_count * width * units, 4 * width * units, row_count * units),
        name="next_branch",
    )(x_next, weights, value_next, conv_taps, conv_bias.reshape(1, units))


def high_and_low(rows):
    high = rows.astype(jnp.bfloat16).astype(jnp.float32)
    return jnp.concatenate([high, rows - high], axis=0).astype(jnp.bfloat16)


def turned_columns(x, parts):
    row_count, width = x.shape
    each = width // parts

    def body(x_ref, out_ref):
        out_ref[...] = x_ref[...].T

    return pl.pallas_call(
        body,
        grid=(parts,),
        in_specs=[pl.BlockSpec((row_count, each), lambda i: (0, i))],
        out_specs=pl.BlockSpec((each, row_count), lambda i: (i, 0)),
        out_shape=jax.ShapeDtypeStruct((width, row_count), x.dtype),
        cost_estimate=cost(2 * row_count * row_count * width, 4 * x.size),
        name="turned_columns",
    )(x)


def weight_gradient(x_turned, grad_up, small, grad_scale, n_zm, n_zq, n_y):
    width, row_count = x_turned.shape
    units = grad_up.shape[1]
    each = width // n_y
    shard_rows = each // (n_zm * n_zq)

    def body(x_ref, g_ref, small_ref, out_ref):
        grad = jnp.dot(
            x_ref[...].reshape(each, row_count), g_ref[...], preferred_element_type=jnp.float32
        )
        grad = (grad * grad_scale).astype(jnp.bfloat16)
        for q in range(n_zq):
            for m in range(n_zm):
                to, at = (q * n_zm + m) * shard_rows, (m * n_zq + q) * shard_rows
                out_ref[0, to : to + shard_rows] = grad[at : at + shard_rows]
        out_ref[0, each:] = high_and_low(small_ref[...] * grad_scale)

    return pl.pallas_call(
        body,
        grid=(n_y,),
        in_specs=[
            pl.BlockSpec((n_zm * n_zq, 1, shard_rows, row_count), lambda i: (0, i, 0, 0)),
            whole(grad_up.shape),
            whole(small.shape),
        ],
        out_specs=pl.BlockSpec((1, each + 2 * SMALL_ROWS, units), lambda i: (i, 0, 0)),
        out_shape=jax.ShapeDtypeStruct((n_y, each + 2 * SMALL_ROWS, units), jnp.bfloat16),
        cost_estimate=cost(2 * row_count * width * units, 4 * width * units),
        name="weight_gradient",
    )(x_turned.reshape(n_zm * n_zq, n_y, shard_rows, row_count), grad_up, small)


def summed(block):
    return jnp.sum(block.astype(jnp.float32), axis=0)


def small_total(block):
    total = summed(block)
    return total[:SMALL_ROWS] + total[SMALL_ROWS:]


def sum_and_repack(arrived, parts, repeats):
    count, rows, units = arrived.shape
    extra = 2 * SMALL_ROWS
    each = (rows - extra) // parts

    def body(main_ref, small_ref, out_ref):
        main = summed(main_ref[...]).astype(jnp.bfloat16)
        small = high_and_low(small_total(small_ref[...]))
        for r in range(repeats):
            out_ref[r, 0, :each] = main
            out_ref[r, 0, each:] = small

    out = pl.pallas_call(
        body,
        grid=(parts,),
        in_specs=[
            pl.BlockSpec((count, each, units), lambda i: (0, i, 0)),
            pl.BlockSpec((count, extra, units), lambda i: (0, (rows - extra) // extra, 0)),
        ],
        out_specs=pl.BlockSpec((repeats, 1, each + extra, units), lambda i: (0, i, 0, 0)),
        out_shape=jax.ShapeDtypeStruct((repeats, parts, each + extra, units), jnp.bfloat16),
        cost_estimate=cost(2 * arrived.size, 4 * arrived.size),
        name="sum_and_repack",
    )(arrived, arrived)
    return out.reshape(repeats * parts, each + extra, units)


def last_sum(arrived, sum_w, sum_taps, sum_bias):
    rows, units = sum_w.shape
    tap_count = sum_taps.shape[0]

    def body(in_ref, w_ref, taps_ref, bias_ref, new_w_ref, new_taps_ref, new_bias_ref):
        new_w_ref[...] = w_ref[...] + summed(in_ref[:, :rows])
        small = small_total(in_ref[:, rows:])
        new_taps_ref[...] = taps_ref[...] + small[:tap_count]
        new_bias_ref[...] = bias_ref[...] + small[tap_count : tap_count + 1]

    new_w, new_taps, new_bias = pl.pallas_call(
        body,
        out_shape=[
            jax.ShapeDtypeStruct(sum_w.shape, jnp.float32),
            jax.ShapeDtypeStruct(sum_taps.shape, jnp.float32),
            jax.ShapeDtypeStruct((1, units), jnp.float32),
        ],
        cost_estimate=cost(2 * arrived.size, 4 * arrived.size),
        name="last_sum",
    )(arrived, sum_w, sum_taps, sum_bias.reshape(1, units))
    return new_w, new_taps, new_bias.reshape(units)


def per_device(
    x_next,
    value_next,
    x_prev,
    value_prev,
    cotangent,
    w_gate,
    conv_taps,
    conv_bias,
    sum_w,
    sum_taps,
    sum_bias,
):
    row_count, width = x_next.shape
    n_zh, n_zm, n_zq, n_y = (lax.axis_size(a) for a in ("zh", "zm", "zq", "y"))
    n_x, n_c = lax.axis_size("x"), lax.axis_size("c")

    pair = copies_to(w_gate, "zm", n_zm)
    quad = copies_to(pair, "zq", n_zq)
    x_turned = turned_columns(x_prev, 8)
    quad, x_turned = lax.optimization_barrier((quad, x_turned))
    plane = copies_to(quad, "y", n_y)

    grad_value, grad_up, small, gathered, turned, to_core = previous_branch(
        x_prev, plane, cotangent, value_prev, conv_taps, conv_bias, n_c
    )
    from_core = send_on(to_core, "c", 1)
    grad_scale = float(row_count * n_zh * n_zm * n_zq * n_y) ** (-0.5)
    by_y = weight_gradient(x_turned, grad_up, small, grad_scale, n_zm, n_zq, n_y)
    by_y, turned = lax.optimization_barrier((by_y, turned))
    from_y = exchange(by_y, "y")

    block_rows = row_count // (n_x * n_c)
    kept = lax.dot_general(
        turned[1], gathered, (((1,), (1,)), ((), ())), preferred_element_type=jnp.float32
    )
    half = (kept + from_core.astype(jnp.float32)).astype(jnp.bfloat16)
    half = half.reshape(n_x, block_rows, width)
    arrived = [half[0]] + [send_on(half[k], "x", k) for k in range(1, n_x)]
    from_y, *arrived = lax.optimization_barrier((from_y, *arrived))
    eighth = sum(block.astype(jnp.float32) for block in arrived).astype(jnp.bfloat16)
    spread = [eighth]
    for k in range(1, n_x):
        spread.append(send_on(eighth, "x", k))

    from_q = exchange(sum_and_repack(from_y, n_zq, 1), "zq")
    by_half = sum_and_repack(from_q, n_zm, n_zh)
    by_half, x_next = lax.optimization_barrier((by_half, x_next))
    from_half = exchange(by_half, ("zh", "zm"))
    hidden_next = next_branch(x_next, gathered, value_next, conv_taps, conv_bias)
    hidden_next, *spread = lax.optimization_barrier((hidden_next, *spread))
    other = [send_on(block, "c", 1) for block in spread]
    from_half, *other = lax.optimization_barrier((from_half, *other))
    grad_input = put_in_order(spread, other, n_c).reshape(row_count, width)
    new_w, new_taps, new_bias = last_sum(from_half, sum_w, sum_taps, sum_bias)
    return hidden_next, grad_input, grad_value, new_w, new_taps, new_bias


def solution(mesh):
    n_fs, n_tp = mesh.shape["fs"], mesh.shape["tp"]
    n_y, n_zq, n_c = 4, 4, 2
    fine = Mesh(
        mesh.devices.reshape(
            mesh.shape["rep"], n_fs // (n_y * n_zq), n_zq, n_y, n_tp // n_c, n_c
        ),
        ("zh", "zm", "zq", "y", "x", "c"),
    )
    fs, tp = ("zm", "zq", "y"), ("x", "c")
    tokens = ("zh", *fs)
    in_specs = (
        P(tokens, None),
        P(tokens, tp),
        P(tokens, None),
        P(tokens, tp),
        P(tokens, tp),
        P(fs, tp),
        P(None, tp),
        P(tp),
        P(fs, tp),
        P(None, tp),
        P(tp),
    )
    out_specs = (
        P(tokens, tp),
        P(tokens, None),
        P(tokens, tp),
        P(fs, tp),
        P(None, tp),
        P(tp),
    )
    return jax.shard_map(
        per_device, mesh=fine, in_specs=in_specs, out_specs=out_specs, check_vma=False
    )
```

```python
import jax
import jax.numpy as jnp
from jax import lax
from jax.experimental import pallas as pl
from jax.experimental.pallas import tpu as pltpu
from jax.sharding import Mesh
from jax.sharding import PartitionSpec as P


SEQ_LEN = 128
SMALL_ROWS = 8


def copies_to(block, axis, size):
    copies = jnp.broadcast_to(block, (size, *block.shape))
    return lax.all_to_all(copies, axis, 0, 0, tiled=True)


def exchange(blocks, axis):
    return lax.all_to_all(blocks, axis, 0, 0, tiled=True)


def send_on(block, axis, shift):
    size = lax.axis_size(axis)
    return lax.ppermute(block, axis, [(i, (i + shift) % size) for i in range(size)])


def near(array):
    return pltpu.with_memory_space_constraint(array, pltpu.VMEM)


VMEM = pl.BlockSpec(memory_space=pltpu.VMEM)
HBM = pl.BlockSpec(memory_space=pltpu.HBM)


def cost(flops, count, exps=0):
    return pl.CostEstimate(flops=flops, bytes_accessed=count, transcendentals=exps)


def put_in_order(own, other, n_c):
    n_x = len(own)
    rows, width = own[0].shape

    def body(*refs):
        out_ref = refs[-1]
        at_x, at_c = lax.axis_index("x"), lax.axis_index("c")
        for k in range(n_x):
            spot = (at_x + n_x - k) % n_x
            out_ref[at_c * n_x + spot] = refs[k][...]
            out_ref[(1 - at_c) * n_x + spot] = refs[n_x + k][...]

    return pl.pallas_call(
        body,
        in_specs=[VMEM] * (2 * n_x),
        out_shape=jax.ShapeDtypeStruct((n_c * n_x, rows, width), own[0].dtype),
        cost_estimate=cost(0, 32 * own[0].size),
        name="put_in_order",
        compiler_params=pltpu.CompilerParams(vmem_limit_bytes=24 * 2**20),
    )(*(near(block) for block in (*own, *other)))


def later(values, offset):
    if offset == 0:
        return values
    rows = lax.broadcasted_iota(jnp.int32, values.shape, 0) % SEQ_LEN
    return jnp.where(rows >= offset, pltpu.roll(values, offset, 0), 0.0)


def earlier(values, offset):
    if offset == 0:
        return values
    count = values.shape[0]
    rows = lax.broadcasted_iota(jnp.int32, values.shape, 0) % SEQ_LEN
    return jnp.where(rows < SEQ_LEN - offset, pltpu.roll(values, count - offset, 0), 0.0)


def gated(up, taps_ref, bias_ref):
    tap_count = taps_ref.shape[0]
    total = bias_ref[...][None, :]
    for j in range(tap_count):
        total = total + taps_ref[j : j + 1, :] * later(up, tap_count - 1 - j)
    return total


def high_and_low(rows):
    high = rows.astype(jnp.bfloat16).astype(jnp.float32)
    return jnp.concatenate([high, rows - high], axis=0).astype(jnp.bfloat16)


def previous_branch(x_prev, plane, cotangent, value_prev, conv_taps, conv_bias, grad_scale, n_c):
    row_count, width = x_prev.shape
    n_y, n_zq, n_zm, shard_rows, units = plane.shape
    tap_count = conv_taps.shape[0]
    n_x = lax.axis_size("x")
    half_rows = row_count // n_c
    block_rows = half_rows // n_x
    each = width // n_y

    def body(
        x_ref,
        w_ref,
        cot_ref,
        value_ref,
        taps_ref,
        bias_ref,
        gv_ref,
        natural_ref,
        keep_ref,
        send_ref,
        by_y_out,
        gu_ref,
        turned_ref,
        by_y_ref,
        sems,
    ):
        spots = [
            (y, q, m, ((m * n_zq + q) * n_y + y) * shard_rows)
            for y in range(n_y)
            for q in range(n_zq)
            for m in range(n_zm)
        ]
        own_half = lax.axis_index("zm")
        for y in range(n_y):
            for q in range(n_zq):
                for m in range(n_zm):
                    half_at = (own_half + m) % n_zm
                    at = ((half_at * n_zq + q) * n_y + y) * shard_rows
                    natural_ref[pl.ds(pl.multiple_of(at, shard_rows), shard_rows)] = w_ref[y, q, m]
        up = jnp.dot(x_ref[...], natural_ref[...], preferred_element_type=jnp.float32)
        up = up.astype(jnp.bfloat16).astype(jnp.float32)
        gate = gated(up, taps_ref, bias_ref)
        sig = jax.nn.sigmoid(gate)
        cot = cot_ref[...].astype(jnp.float32)
        gv_ref[...] = (cot * gate * sig).astype(jnp.bfloat16)
        grad_gate = cot * value_ref[...].astype(jnp.float32) * sig * (1.0 + gate * (1.0 - sig))
        grad_up = jnp.zeros_like(grad_gate)
        for j in range(tap_count):
            grad_up = grad_up + taps_ref[j : j + 1, :] * earlier(grad_gate, tap_count - 1 - j)
        gu_ref[...] = grad_up.astype(jnp.bfloat16)

        at_x, at_c = lax.axis_index("x"), lax.axis_index("c")
        for i, half_ref in ((1, turned_ref), (0, keep_ref)):
            core = (at_c + i) % n_c
            for k in range(n_x):
                row = core * half_rows + ((at_x + k) % n_x) * block_rows
                half_ref[k * block_rows : (k + 1) * block_rows] = gu_ref[
                    pl.ds(pl.multiple_of(row, block_rows), block_rows)
                ]
        send_ref[...] = lax.dot_general(
            turned_ref[...],
            natural_ref[...],
            (((1,), (1,)), ((), ())),
            preferred_element_type=jnp.float32,
        ).astype(jnp.bfloat16)

        grad_w = lax.dot_general(
            x_ref[...], gu_ref[...], (((0,), (0,)), ((), ())), preferred_element_type=jnp.float32
        )
        grad_w = (grad_w * grad_scale).astype(jnp.bfloat16)
        sums = [
            jnp.sum(grad_gate * later(up, tap_count - 1 - j), axis=0, keepdims=True)
            for j in range(tap_count)
        ] + [jnp.sum(grad_gate, axis=0, keepdims=True)]
        rest = jnp.zeros((SMALL_ROWS - len(sums), units), jnp.float32)
        small = high_and_low(jnp.concatenate([*sums, rest], axis=0) * grad_scale)
        moves = []
        for y in range(n_y):
            for at_y, q, m, at in spots:
                if at_y == y:
                    to = (q * n_zm + m) * shard_rows
                    by_y_ref[y, to : to + shard_rows] = grad_w[at : at + shard_rows]
            by_y_ref[y, each:] = small
            moves.append(pltpu.make_async_copy(by_y_ref.at[y], by_y_out.at[y], sems.at[y]))
            moves[-1].start()
        for move in moves:
            move.wait()

    half = jnp.bfloat16
    return pl.pallas_call(
        body,
        in_specs=[VMEM] * 6,
        out_specs=[pl.BlockSpec(), VMEM, VMEM, pl.BlockSpec(), HBM],
        out_shape=[
            jax.ShapeDtypeStruct((row_count, units), half),
            pltpu.VMEM((width, units), half),
            pltpu.VMEM((half_rows, units), half),
            jax.ShapeDtypeStruct((half_rows, width), half),
            pltpu.HBM((n_y, each + 2 * SMALL_ROWS, units), half),
        ],
        scratch_shapes=[
            pltpu.VMEM((row_count, units), half),
            pltpu.VMEM((half_rows, units), half),
            pltpu.VMEM((n_y, each + 2 * SMALL_ROWS, units), half),
            pltpu.SemaphoreType.DMA((n_y,)),
        ],
        cost_estimate=cost(5 * row_count * width * units, 8 * width * units, row_count * units),
        name="previous_branch",
        compiler_params=pltpu.CompilerParams(vmem_limit_bytes=24 * 2**20),
    )(
        near(x_prev),
        near(plane),
        near(cotangent),
        near(value_prev),
        near(conv_taps),
        near(conv_bias),
    )


def next_branch(x_next, weights, value_next, conv_taps, conv_bias):
    row_count, width = x_next.shape
    units = weights.shape[1]

    def body(x_ref, w_ref, value_ref, taps_ref, bias_ref, out_ref):
        up = jnp.dot(x_ref[...], w_ref[...], preferred_element_type=jnp.float32)
        gate = gated(up.astype(jnp.bfloat16).astype(jnp.float32), taps_ref, bias_ref)
        hidden = gate * jax.nn.sigmoid(gate) * value_ref[...].astype(jnp.float32)
        out_ref[...] = hidden.astype(jnp.bfloat16)

    return pl.pallas_call(
        body,
        in_specs=[VMEM] * 5,
        out_shape=jax.ShapeDtypeStruct((row_count, units), jnp.bfloat16),
        cost_estimate=cost(2 * row_count * width * units, 4 * width * units, row_count * units),
        name="next_branch",
        compiler_params=pltpu.CompilerParams(vmem_limit_bytes=24 * 2**20),
    )(near(x_next), near(weights), near(value_next), near(conv_taps), near(conv_bias))


def summed(block):
    return jnp.sum(block.astype(jnp.float32), axis=0)


def small_total(block):
    total = summed(block)
    return total[:SMALL_ROWS] + total[SMALL_ROWS:]


def sum_and_repack(arrived, parts, repeats):
    _, rows, units = arrived.shape
    extra = 2 * SMALL_ROWS
    each = (rows - extra) // parts

    def body(in_ref, out_ref, block_ref, sems):
        small = high_and_low(small_total(in_ref[:, rows - extra :]))
        moves = []
        for p in range(parts):
            main = summed(in_ref[:, p * each : (p + 1) * each]).astype(jnp.bfloat16)
            block_ref[p, :each] = main
            block_ref[p, each:] = small
            for r in range(repeats):
                to = r * parts + p
                move = pltpu.make_async_copy(block_ref.at[p], out_ref.at[to], sems.at[to])
                move.start()
                moves.append(move)
        for move in moves:
            move.wait()

    return pl.pallas_call(
        body,
        in_specs=[VMEM],
        out_specs=HBM,
        out_shape=pltpu.HBM((repeats * parts, each + extra, units), jnp.bfloat16),
        scratch_shapes=[
            pltpu.VMEM((parts, each + extra, units), jnp.bfloat16),
            pltpu.SemaphoreType.DMA((repeats * parts,)),
        ],
        cost_estimate=cost(2 * arrived.size, 4 * arrived.size),
        name="sum_and_repack",
        compiler_params=pltpu.CompilerParams(vmem_limit_bytes=24 * 2**20),
    )(near(arrived))


def last_sum(arrived, sum_w, sum_taps, sum_bias):
    rows, _ = sum_w.shape
    tap_count = sum_taps.shape[0]

    def body(in_ref, w_ref, taps_ref, bias_ref, new_w_ref, new_taps_ref, new_bias_ref):
        new_w_ref[...] = w_ref[...] + summed(in_ref[:, :rows])
        small = small_total(in_ref[:, rows:])
        new_taps_ref[...] = taps_ref[...] + small[:tap_count]
        new_bias_ref[...] = bias_ref[...] + small[tap_count]

    return pl.pallas_call(
        body,
        in_specs=[VMEM] * 4,
        out_shape=[
            jax.ShapeDtypeStruct(sum_w.shape, jnp.float32),
            jax.ShapeDtypeStruct(sum_taps.shape, jnp.float32),
            jax.ShapeDtypeStruct(sum_bias.shape, jnp.float32),
        ],
        cost_estimate=cost(2 * arrived.size, 4 * arrived.size),
        name="last_sum",
        compiler_params=pltpu.CompilerParams(vmem_limit_bytes=24 * 2**20),
    )(near(arrived), near(sum_w), near(sum_taps), near(sum_bias))


def per_device(
    x_next,
    value_next,
    x_prev,
    value_prev,
    cotangent,
    w_gate,
    conv_taps,
    conv_bias,
    sum_w,
    sum_taps,
    sum_bias,
):
    row_count, width = x_next.shape
    n_zh, n_zm, n_zq, n_y = (lax.axis_size(a) for a in ("zh", "zm", "zq", "y"))
    n_x, n_c = lax.axis_size("x"), lax.axis_size("c")

    pair = jnp.stack([w_gate, send_on(w_gate, "zm", 1)])
    quad = copies_to(pair, "zq", n_zq)
    plane = copies_to(quad, "y", n_y)
    grad_scale = float(row_count * n_zh * n_zm * n_zq * n_y) ** (-0.5)
    grad_value, gathered, keep, to_core, by_y = previous_branch(
        x_prev, plane, cotangent, value_prev, conv_taps, conv_bias, grad_scale, n_c
    )
    from_core = send_on(to_core, "c", 1)
    from_y = exchange(by_y, "y")

    block_rows = row_count // (n_x * n_c)
    kept = lax.dot_general(
        keep, gathered, (((1,), (1,)), ((), ())), preferred_element_type=jnp.float32
    )
    half = (kept + from_core.astype(jnp.float32)).astype(jnp.bfloat16)
    half = half.reshape(n_x, block_rows, width)
    arrived = [half[0]] + [send_on(half[k], "x", k) for k in range(1, n_x)]
    from_y, *arrived = lax.optimization_barrier((from_y, *arrived))
    eighth = sum(block.astype(jnp.float32) for block in arrived).astype(jnp.bfloat16)
    spread = [eighth]
    for k in range(1, n_x):
        spread.append(send_on(eighth, "x", k))

    from_q = exchange(sum_and_repack(from_y, n_zq, 1), "zq")
    by_half = sum_and_repack(from_q, n_zm, n_zh)
    by_half, x_next = lax.optimization_barrier((by_half, x_next))
    from_half = exchange(by_half, ("zh", "zm"))
    hidden_next = next_branch(x_next, gathered, value_next, conv_taps, conv_bias)
    hidden_next, *spread = lax.optimization_barrier((hidden_next, *spread))
    other = [send_on(block, "c", 1) for block in spread]
    grad_input = put_in_order(spread, other, n_c).reshape(row_count, width)
    from_half, grad_input = lax.optimization_barrier((from_half, grad_input))
    new_w, new_taps, new_bias = last_sum(from_half, sum_w, sum_taps, sum_bias)
    return hidden_next, grad_input, grad_value, new_w, new_taps, new_bias


def solution(mesh):
    n_fs, n_tp = mesh.shape["fs"], mesh.shape["tp"]
    n_y, n_zq, n_c = 4, 4, 2
    fine = Mesh(
        mesh.devices.reshape(
            mesh.shape["rep"], n_fs // (n_y * n_zq), n_zq, n_y, n_tp // n_c, n_c
        ),
        ("zh", "zm", "zq", "y", "x", "c"),
    )
    fs, tp = ("zm", "zq", "y"), ("x", "c")
    tokens = ("zh", *fs)
    in_specs = (
        P(tokens, None),
        P(tokens, tp),
        P(tokens, None),
        P(tokens, tp),
        P(tokens, tp),
        P(fs, tp),
        P(None, tp),
        P(tp),
        P(fs, tp),
        P(None, tp),
        P(tp),
    )
    out_specs = (
        P(tokens, tp),
        P(tokens, None),
        P(tokens, tp),
        P(fs, tp),
        P(None, tp),
        P(tp),
    )
    return jax.shard_map(
        per_device, mesh=fine, in_specs=in_specs, out_specs=out_specs, check_vma=False
    )
```

```python
import jax
import jax.numpy as jnp
from jax import lax
from jax.experimental import pallas as pl
from jax.experimental.pallas import tpu as pltpu
from jax.sharding import Mesh
from jax.sharding import PartitionSpec as P

SEQ_LEN = 128
SMALL_ROWS = 8
FAR, NEAR = ("zm", "zp"), ("zl", "y")


def copies_to(block, axis, size):
    copies = jnp.broadcast_to(block, (size, *block.shape))
    return lax.all_to_all(copies, axis, 0, 0, tiled=True)


def exchange(blocks, axis):
    return lax.all_to_all(blocks, axis, 0, 0, tiled=True)


def send_on(block, axis, shift):
    size = lax.axis_size(axis)
    return lax.ppermute(block, axis, [(i, (i + shift) % size) for i in range(size)])


def whole(shape):
    return pl.BlockSpec(shape, lambda *_: (0,) * len(shape))


def near(array):
    return pltpu.with_memory_space_constraint(array, pltpu.VMEM)


VMEM = pl.BlockSpec(memory_space=pltpu.VMEM)
HBM = pl.BlockSpec(memory_space=pltpu.HBM)


def cost(flops, count, exps=0):
    return pl.CostEstimate(flops=flops, bytes_accessed=count, transcendentals=exps)


def put_in_order(own, other, n_c):
    n_x = len(own)
    rows, width = own[0].shape

    def body(*refs):
        out_ref = refs[-1]
        at_x, at_c = lax.axis_index("x"), lax.axis_index("c")
        for k in range(n_x):
            spot = (at_x + n_x - k) % n_x
            out_ref[at_c * n_x + spot] = refs[k][...]
            out_ref[(1 - at_c) * n_x + spot] = refs[n_x + k][...]

    return pl.pallas_call(
        body,
        in_specs=[VMEM] * (2 * n_x),
        out_shape=jax.ShapeDtypeStruct((n_c * n_x, rows, width), own[0].dtype),
        cost_estimate=cost(0, 32 * own[0].size),
        name="put_in_order",
        compiler_params=pltpu.CompilerParams(vmem_limit_bytes=24 * 2**20),
    )(*(near(block) for block in (*own, *other)))


def later(values, offset):
    if offset == 0:
        return values
    rows = lax.broadcasted_iota(jnp.int32, values.shape, 0) % SEQ_LEN
    return jnp.where(rows >= offset, pltpu.roll(values, offset, 0), 0.0)


def earlier(values, offset):
    if offset == 0:
        return values
    count = values.shape[0]
    rows = lax.broadcasted_iota(jnp.int32, values.shape, 0) % SEQ_LEN
    return jnp.where(rows < SEQ_LEN - offset, pltpu.roll(values, count - offset, 0), 0.0)


def gated(up, taps_ref, bias_ref):
    tap_count = taps_ref.shape[0]
    total = bias_ref[...][None, :]
    for j in range(tap_count):
        total = total + taps_ref[j : j + 1, :] * later(up, tap_count - 1 - j)
    return total


def high_and_low(rows):
    high = rows.astype(jnp.bfloat16).astype(jnp.float32)
    half = SMALL_ROWS // 2
    return (high + pltpu.roll(rows - high, half, 0)).astype(jnp.bfloat16)


def previous_branch(x_prev, plane, cotangent, value_prev, conv_taps, conv_bias, grad_scale, n_c):
    row_count, width = x_prev.shape
    n_near, n_far, shard_rows, units = plane.shape
    tap_count = conv_taps.shape[0]
    n_x = lax.axis_size("x")
    half_rows = row_count // n_c
    block_rows = half_rows // n_x
    each = n_far * shard_rows

    def body(
        x_ref,
        w_ref,
        cot_ref,
        value_ref,
        taps_ref,
        bias_ref,
        gv_ref,
        natural_ref,
        keep_ref,
        send_ref,
        sent_out,
        gu_ref,
        turned_ref,
        sent_ref,
        sems,
    ):
        spots = [
            (near_at, far_at, (far_at * n_near + near_at) * shard_rows)
            for near_at in range(n_near)
            for far_at in range(n_far)
        ]
        for near_at, far_at, at in spots:
            natural_ref[at : at + shard_rows] = w_ref[near_at, far_at]
        up = jnp.dot(x_ref[...], natural_ref[...], preferred_element_type=jnp.float32)
        up = up.astype(jnp.bfloat16).astype(jnp.float32)
        gate = gated(up, taps_ref, bias_ref)
        sig = jax.nn.sigmoid(gate)
        cot = cot_ref[...].astype(jnp.float32)
        gv_ref[...] = (cot * gate * sig).astype(jnp.bfloat16)
        grad_gate = cot * value_ref[...].astype(jnp.float32) * sig * (1.0 + gate * (1.0 - sig))
        grad_up = jnp.zeros_like(grad_gate)
        for j in range(tap_count):
            grad_up = grad_up + taps_ref[j : j + 1, :] * earlier(grad_gate, tap_count - 1 - j)
        gu_ref[...] = grad_up.astype(jnp.bfloat16)

        at_x, at_c = lax.axis_index("x"), lax.axis_index("c")
        for i, half_ref in ((1, turned_ref), (0, keep_ref)):
            core = (at_c + i) % n_c
            for k in range(n_x):
                row = core * half_rows + ((at_x + k) % n_x) * block_rows
                half_ref[k * block_rows : (k + 1) * block_rows] = gu_ref[
                    pl.ds(pl.multiple_of(row, block_rows), block_rows)
                ]
        send_ref[...] = lax.dot_general(
            turned_ref[...],
            natural_ref[...],
            (((1,), (1,)), ((), ())),
            preferred_element_type=jnp.float32,
        ).astype(jnp.bfloat16)

        grad_w = lax.dot_general(
            x_ref[...], gu_ref[...], (((0,), (0,)), ((), ())), preferred_element_type=jnp.float32
        )
        grad_w = (grad_w * grad_scale).astype(jnp.bfloat16)
        sums = [
            jnp.sum(grad_gate * later(up, tap_count - 1 - j), axis=0, keepdims=True)
            for j in range(tap_count)
        ] + [jnp.sum(grad_gate, axis=0, keepdims=True)]
        rest = jnp.zeros((SMALL_ROWS - len(sums), units), jnp.float32)
        small = high_and_low(jnp.concatenate([*sums, rest], axis=0) * grad_scale)
        moves = []
        for block in range(n_near):
            for near_at, far_at, at in spots:
                if near_at == block:
                    to = far_at * shard_rows
                    sent_ref[block, to : to + shard_rows] = grad_w[at : at + shard_rows]
            sent_ref[block, each:] = small
            moves.append(
                pltpu.make_async_copy(sent_ref.at[block], sent_out.at[block], sems.at[block])
            )
            moves[-1].start()
        for move in moves:
            move.wait()

    half = jnp.bfloat16
    return pl.pallas_call(
        body,
        in_specs=[VMEM] * 6,
        out_specs=[pl.BlockSpec(), VMEM, VMEM, pl.BlockSpec(), HBM],
        out_shape=[
            jax.ShapeDtypeStruct((row_count, units), half),
            pltpu.VMEM((width, units), half),
            pltpu.VMEM((half_rows, units), half),
            jax.ShapeDtypeStruct((half_rows, width), half),
            pltpu.HBM((n_near, each + SMALL_ROWS, units), half),
        ],
        scratch_shapes=[
            pltpu.VMEM((row_count, units), half),
            pltpu.VMEM((half_rows, units), half),
            pltpu.VMEM((n_near, each + SMALL_ROWS, units), half),
            pltpu.SemaphoreType.DMA((n_near,)),
        ],
        cost_estimate=cost(5 * row_count * width * units, 8 * width * units, row_count * units),
        name="previous_branch",
        compiler_params=pltpu.CompilerParams(vmem_limit_bytes=24 * 2**20),
    )(
        near(x_prev),
        near(plane),
        near(cotangent),
        near(value_prev),
        near(conv_taps),
        near(conv_bias),
    )


def next_branch(x_next, weights, value_next, conv_taps, conv_bias):
    row_count, width = x_next.shape
    units = weights.shape[1]

    def body(x_ref, w_ref, value_ref, taps_ref, bias_ref, out_ref):
        up = jnp.dot(x_ref[...], w_ref[...], preferred_element_type=jnp.float32)
        gate = gated(up.astype(jnp.bfloat16).astype(jnp.float32), taps_ref, bias_ref)
        hidden = gate * jax.nn.sigmoid(gate) * value_ref[...].astype(jnp.float32)
        out_ref[...] = hidden.astype(jnp.bfloat16)

    return pl.pallas_call(
        body,
        in_specs=[VMEM] * 5,
        out_shape=jax.ShapeDtypeStruct((row_count, units), jnp.bfloat16),
        cost_estimate=cost(2 * row_count * width * units, 4 * width * units, row_count * units),
        name="next_branch",
        compiler_params=pltpu.CompilerParams(vmem_limit_bytes=24 * 2**20),
    )(near(x_next), near(weights), near(value_next), near(conv_taps), near(conv_bias))


def summed(block):
    return jnp.sum(block.astype(jnp.float32), axis=0)


def small_total(block):
    total = summed(block)
    half = SMALL_ROWS // 2
    rows = lax.broadcasted_iota(jnp.int32, total.shape, 0)
    return jnp.where(rows < half, total + pltpu.roll(total, half, 0), 0.0)


def sum_and_repack(arrived, parts, repeats):
    count, rows, units = arrived.shape
    extra = SMALL_ROWS
    each = (rows - extra) // parts

    def body(in_ref, out_ref, block_ref, sems):
        small = high_and_low(small_total(in_ref[:, rows - extra :]))
        moves = []
        for p in range(parts):
            main = summed(in_ref[:, p * each : (p + 1) * each]).astype(jnp.bfloat16)
            block_ref[p, :each] = main
            block_ref[p, each:] = small
            for r in range(repeats):
                to = r * parts + p
                move = pltpu.make_async_copy(block_ref.at[p], out_ref.at[to], sems.at[to])
                move.start()
                moves.append(move)
        for move in moves:
            move.wait()

    return pl.pallas_call(
        body,
        in_specs=[VMEM],
        out_specs=HBM,
        out_shape=pltpu.HBM((repeats * parts, each + extra, units), jnp.bfloat16),
        scratch_shapes=[
            pltpu.VMEM((parts, each + extra, units), jnp.bfloat16),
            pltpu.SemaphoreType.DMA((repeats * parts,)),
        ],
        cost_estimate=cost(2 * arrived.size, 4 * arrived.size),
        name="sum_and_repack",
        compiler_params=pltpu.CompilerParams(vmem_limit_bytes=24 * 2**20),
    )(near(arrived))


def last_sum(arrived, sum_w, sum_taps, sum_bias):
    rows, units = sum_w.shape
    tap_count = sum_taps.shape[0]

    def body(in_ref, w_ref, taps_ref, bias_ref, new_w_ref, new_taps_ref, new_bias_ref):
        new_w_ref[...] = w_ref[...] + summed(in_ref[:, :rows])
        small = small_total(in_ref[:, rows:])
        new_taps_ref[...] = taps_ref[...] + small[:tap_count]
        new_bias_ref[...] = bias_ref[...] + small[tap_count]

    return pl.pallas_call(
        body,
        in_specs=[VMEM] * 4,
        out_shape=[
            jax.ShapeDtypeStruct(sum_w.shape, jnp.float32),
            jax.ShapeDtypeStruct(sum_taps.shape, jnp.float32),
            jax.ShapeDtypeStruct(sum_bias.shape, jnp.float32),
        ],
        cost_estimate=cost(2 * arrived.size, 4 * arrived.size),
        name="last_sum",
        compiler_params=pltpu.CompilerParams(vmem_limit_bytes=24 * 2**20),
    )(near(arrived), near(sum_w), near(sum_taps), near(sum_bias))


def per_device(
    x_next,
    value_next,
    x_prev,
    value_prev,
    cotangent,
    w_gate,
    conv_taps,
    conv_bias,
    sum_w,
    sum_taps,
    sum_bias,
):
    row_count, width = x_next.shape
    shard_rows, units = w_gate.shape
    n_zh, n_x, n_c = (lax.axis_size(a) for a in ("zh", "x", "c"))
    n_far, n_near = lax.axis_size(FAR), lax.axis_size(NEAR)

    plane = copies_to(copies_to(w_gate, FAR, n_far), NEAR, n_near)
    grad_scale = float(row_count * n_zh * n_far * n_near) ** (-0.5)
    grad_value, gathered, keep, to_core, sent = previous_branch(
        x_prev, plane, cotangent, value_prev, conv_taps, conv_bias, grad_scale, n_c
    )
    from_core = send_on(to_core, "c", 1)
    from_near = exchange(sent, NEAR)

    block_rows = row_count // (n_x * n_c)
    kept = lax.dot_general(
        keep, gathered, (((1,), (1,)), ((), ())), preferred_element_type=jnp.float32
    )
    half = (kept + from_core.astype(jnp.float32)).astype(jnp.bfloat16)
    half = half.reshape(n_x, block_rows, width)
    arrived = [half[0]] + [send_on(half[k], "x", k) for k in range(1, n_x)]
    hidden_next = next_branch(x_next, gathered, value_next, conv_taps, conv_bias)
    from_near, hidden_next, *arrived = lax.optimization_barrier((from_near, hidden_next, *arrived))
    eighth = sum(block.astype(jnp.float32) for block in arrived).astype(jnp.bfloat16)
    spread = [eighth] + [send_on(eighth, "x", k) for k in range(1, n_x)]
    other = [send_on(block, "c", 1) for block in spread]
    grad_input = put_in_order(spread, other, n_c).reshape(row_count, width)

    from_far = exchange(sum_and_repack(from_near, n_far, n_zh), ("zh", *FAR))
    from_far, grad_input = lax.optimization_barrier((from_far, grad_input))
    new_w, new_taps, new_bias = last_sum(from_far, sum_w, sum_taps, sum_bias)
    return hidden_next, grad_input, grad_value, new_w, new_taps, new_bias


def solution(mesh):
    n_fs, n_tp = mesh.shape["fs"], mesh.shape["tp"]
    n_y, n_c = 4, 2
    n_z = n_fs // n_y
    fine = Mesh(
        mesh.devices.reshape(mesh.shape["rep"], n_z // 4, 2, 2, n_y, n_tp // n_c, n_c),
        ("zh", *FAR, *NEAR, "x", "c"),
    )
    fs, tp = (*FAR, *NEAR), ("x", "c")
    tokens = ("zh", *fs)
    in_specs = (
        P(tokens, None),
        P(tokens, tp),
        P(tokens, None),
        P(tokens, tp),
        P(tokens, tp),
        P(fs, tp),
        P(None, tp),
        P(tp),
        P(fs, tp),
        P(None, tp),
        P(tp),
    )
    out_specs = (
        P(tokens, tp),
        P(tokens, None),
        P(tokens, tp),
        P(fs, tp),
        P(None, tp),
        P(tp),
    )
    return jax.shard_map(
        per_device, mesh=fine, in_specs=in_specs, out_specs=out_specs, check_vma=False
    )
```

```python
import jax
import jax.numpy as jnp
from jax import lax
from jax.experimental import pallas as pl
from jax.experimental.pallas import tpu as pltpu
from jax.sharding import Mesh
from jax.sharding import PartitionSpec as P


SEQ_LEN = 128
SMALL_ROWS = 8
FAR, NEAR = ("zm", "zp"), ("zl", "y")


def copies_to(block, axis, size):
    copies = jnp.broadcast_to(block, (size, *block.shape))
    return lax.all_to_all(copies, axis, 0, 0, tiled=True)


def exchange(blocks, axis):
    return lax.all_to_all(blocks, axis, 0, 0, tiled=True)


def send_on(block, axis, shift):
    size = lax.axis_size(axis)
    return lax.ppermute(block, axis, [(i, (i + shift) % size) for i in range(size)])


def near(array):
    return pltpu.with_memory_space_constraint(array, pltpu.VMEM)


VMEM = pl.BlockSpec(memory_space=pltpu.VMEM)
HBM = pl.BlockSpec(memory_space=pltpu.HBM)


def cost(flops, count, exps=0):
    return pl.CostEstimate(flops=flops, bytes_accessed=count, transcendentals=exps)


def put_in_order(own, other, n_c):
    n_x = own.shape[0]

    def body(own_ref, other_ref, out_ref):
        at_x, at_c = lax.axis_index("x"), lax.axis_index("c")
        for k in range(n_x):
            spot = (at_x + n_x - k) % n_x
            out_ref[at_c * n_x + spot] = own_ref[k]
            out_ref[(1 - at_c) * n_x + spot] = other_ref[k]

    return pl.pallas_call(
        body,
        in_specs=[VMEM] * 2,
        out_shape=jax.ShapeDtypeStruct((n_c * n_x, *own.shape[1:]), own.dtype),
        cost_estimate=cost(0, 8 * own.size),
        name="put_in_order",
        compiler_params=pltpu.CompilerParams(vmem_limit_bytes=24 * 2**20),
    )(near(own), near(other))


def later(values, offset):
    if offset == 0:
        return values
    rows = lax.broadcasted_iota(jnp.int32, values.shape, 0) % SEQ_LEN
    return jnp.where(rows >= offset, pltpu.roll(values, offset, 0), 0.0)


def earlier(values, offset):
    if offset == 0:
        return values
    count = values.shape[0]
    rows = lax.broadcasted_iota(jnp.int32, values.shape, 0) % SEQ_LEN
    return jnp.where(rows < SEQ_LEN - offset, pltpu.roll(values, count - offset, 0), 0.0)


def gated(up, taps_ref, bias_ref):
    tap_count = taps_ref.shape[0]
    total = bias_ref[...][None, :]
    for j in range(tap_count):
        total = total + taps_ref[j : j + 1, :] * later(up, tap_count - 1 - j)
    return total


def high_and_low(rows):
    high = rows.astype(jnp.bfloat16).astype(jnp.float32)
    half = SMALL_ROWS // 2
    return (high + pltpu.roll(rows - high, half, 0)).astype(jnp.bfloat16)


def previous_branch(x_prev, plane, cotangent, value_prev, conv_taps, conv_bias, n_c):
    row_count, width = x_prev.shape
    n_near, n_far, shard_rows, units = plane.shape
    tap_count = conv_taps.shape[0]
    n_x = lax.axis_size("x")
    half_rows = row_count // n_c
    block_rows = half_rows // n_x

    def body(
        x_ref,
        w_ref,
        cot_ref,
        value_ref,
        taps_ref,
        bias_ref,
        gv_ref,
        natural_ref,
        keep_ref,
        send_out,
        gu_ref,
        small_ref,
        turned_ref,
        send_ref,
        sem,
    ):
        spots = [
            (near_at, far_at, (far_at * n_near + near_at) * shard_rows)
            for near_at in range(n_near)
            for far_at in range(n_far)
        ]
        for near_at, far_at, at in spots:
            natural_ref[at : at + shard_rows] = w_ref[near_at, far_at]
        up = jnp.dot(x_ref[...], natural_ref[...], preferred_element_type=jnp.float32)
        up = up.astype(jnp.bfloat16).astype(jnp.float32)
        gate = gated(up, taps_ref, bias_ref)
        sig = jax.nn.sigmoid(gate)
        cot = cot_ref[...].astype(jnp.float32)
        gv_ref[...] = (cot * gate * sig).astype(jnp.bfloat16)
        grad_gate = cot * value_ref[...].astype(jnp.float32) * sig * (1.0 + gate * (1.0 - sig))
        grad_up = jnp.zeros_like(grad_gate)
        for j in range(tap_count):
            grad_up = grad_up + taps_ref[j : j + 1, :] * earlier(grad_gate, tap_count - 1 - j)
        gu_ref[...] = grad_up.astype(jnp.bfloat16)

        at_x, at_c = lax.axis_index("x"), lax.axis_index("c")
        for i, half_ref in ((1, turned_ref), (0, keep_ref)):
            core = (at_c + i) % n_c
            for k in range(n_x):
                row = core * half_rows + ((at_x + k) % n_x) * block_rows
                half_ref[k * block_rows : (k + 1) * block_rows] = gu_ref[
                    pl.ds(pl.multiple_of(row, block_rows), block_rows)
                ]
        send_ref[...] = lax.dot_general(
            turned_ref[...],
            natural_ref[...],
            (((1,), (1,)), ((), ())),
            preferred_element_type=jnp.float32,
        ).astype(jnp.bfloat16)
        move = pltpu.make_async_copy(send_ref, send_out, sem)
        move.start()
        sums = [
            jnp.sum(grad_gate * later(up, tap_count - 1 - j), axis=0, keepdims=True)
            for j in range(tap_count)
        ] + [jnp.sum(grad_gate, axis=0, keepdims=True)]
        rest = jnp.zeros((SMALL_ROWS - len(sums), units), jnp.float32)
        small_ref[...] = jnp.concatenate([*sums, rest], axis=0)
        move.wait()

    half = jnp.bfloat16
    return pl.pallas_call(
        body,
        in_specs=[VMEM] * 6,
        out_specs=[pl.BlockSpec(), VMEM, VMEM, HBM, VMEM, VMEM],
        out_shape=[
            jax.ShapeDtypeStruct((row_count, units), half),
            pltpu.VMEM((width, units), half),
            pltpu.VMEM((half_rows, units), half),
            pltpu.HBM((half_rows, width), half),
            pltpu.VMEM((row_count, units), half),
            pltpu.VMEM((SMALL_ROWS, units), jnp.float32),
        ],
        scratch_shapes=[
            pltpu.VMEM((half_rows, units), half),
            pltpu.VMEM((half_rows, width), half),
            pltpu.SemaphoreType.DMA(()),
        ],
        cost_estimate=cost(3 * row_count * width * units, 8 * width * units, row_count * units),
        name="previous_branch",
        compiler_params=pltpu.CompilerParams(vmem_limit_bytes=24 * 2**20),
    )(
        near(x_prev),
        near(plane),
        near(cotangent),
        near(value_prev),
        near(conv_taps),
        near(conv_bias),
    )


def weight_gradient(x_prev, grad_up, small, grad_scale, n_near, n_far):
    row_count, width = x_prev.shape
    units = grad_up.shape[1]
    each = width // n_near
    shard_rows = each // n_far

    def body(x_ref, g_ref, small_ref, sent_out, sent_ref, sems):
        grad_w = lax.dot_general(
            x_ref[...], g_ref[...], (((0,), (0,)), ((), ())), preferred_element_type=jnp.float32
        )
        grad_w = (grad_w * grad_scale).astype(jnp.bfloat16)
        last = high_and_low(small_ref[...] * grad_scale)
        moves = []
        for block in range(n_near):
            for far_at in range(n_far):
                at, to = (far_at * n_near + block) * shard_rows, far_at * shard_rows
                sent_ref[block, to : to + shard_rows] = grad_w[at : at + shard_rows]
            sent_ref[block, each:] = last
            moves.append(
                pltpu.make_async_copy(sent_ref.at[block], sent_out.at[block], sems.at[block])
            )
            moves[-1].start()
        for move in moves:
            move.wait()

    shape = (n_near, each + SMALL_ROWS, units)
    return pl.pallas_call(
        body,
        in_specs=[VMEM] * 3,
        out_specs=HBM,
        out_shape=pltpu.HBM(shape, jnp.bfloat16),
        scratch_shapes=[
            pltpu.VMEM(shape, jnp.bfloat16),
            pltpu.SemaphoreType.DMA((n_near,)),
        ],
        cost_estimate=cost(2 * row_count * width * units, 4 * width * units),
        name="weight_gradient",
        compiler_params=pltpu.CompilerParams(vmem_limit_bytes=24 * 2**20),
    )(near(x_prev), near(grad_up), near(small))


def next_branch(x_next, weights, value_next, conv_taps, conv_bias):
    row_count, width = x_next.shape
    units = weights.shape[1]

    def body(x_ref, w_ref, value_ref, taps_ref, bias_ref, out_ref):
        up = jnp.dot(x_ref[...], w_ref[...], preferred_element_type=jnp.float32)
        gate = gated(up.astype(jnp.bfloat16).astype(jnp.float32), taps_ref, bias_ref)
        hidden = gate * jax.nn.sigmoid(gate) * value_ref[...].astype(jnp.float32)
        out_ref[...] = hidden.astype(jnp.bfloat16)

    return pl.pallas_call(
        body,
        in_specs=[VMEM] * 5,
        out_shape=jax.ShapeDtypeStruct((row_count, units), jnp.bfloat16),
        cost_estimate=cost(2 * row_count * width * units, 4 * width * units, row_count * units),
        name="next_branch",
        compiler_params=pltpu.CompilerParams(vmem_limit_bytes=24 * 2**20),
    )(near(x_next), near(weights), near(value_next), near(conv_taps), near(conv_bias))


def summed(block):
    return jnp.sum(block.astype(jnp.float32), axis=0)


def small_total(block):
    total = summed(block)
    half = SMALL_ROWS // 2
    rows = lax.broadcasted_iota(jnp.int32, total.shape, 0)
    return jnp.where(rows < half, total + pltpu.roll(total, half, 0), 0.0)


def sum_and_repack(arrived, parts, repeats):
    _, rows, units = arrived.shape
    extra = SMALL_ROWS
    each = (rows - extra) // parts

    def body(in_ref, out_ref, block_ref, sems):
        small = high_and_low(small_total(in_ref[:, rows - extra :]))
        moves = []
        for p in range(parts):
            main = summed(in_ref[:, p * each : (p + 1) * each]).astype(jnp.bfloat16)
            block_ref[p, :each] = main
            block_ref[p, each:] = small
            for r in range(repeats):
                to = r * parts + p
                move = pltpu.make_async_copy(block_ref.at[p], out_ref.at[to], sems.at[to])
                move.start()
                moves.append(move)
        for move in moves:
            move.wait()

    return pl.pallas_call(
        body,
        in_specs=[VMEM],
        out_specs=HBM,
        out_shape=pltpu.HBM((repeats * parts, each + extra, units), jnp.bfloat16),
        scratch_shapes=[
            pltpu.VMEM((parts, each + extra, units), jnp.bfloat16),
            pltpu.SemaphoreType.DMA((repeats * parts,)),
        ],
        cost_estimate=cost(2 * arrived.size, 4 * arrived.size),
        name="sum_and_repack",
        compiler_params=pltpu.CompilerParams(vmem_limit_bytes=24 * 2**20),
    )(near(arrived))


def last_sum(arrived, sum_w, sum_taps, sum_bias):
    rows, _ = sum_w.shape
    tap_count = sum_taps.shape[0]

    def body(in_ref, w_ref, taps_ref, bias_ref, new_w_ref, new_taps_ref, new_bias_ref):
        new_w_ref[...] = w_ref[...] + summed(in_ref[:, :rows])
        small = small_total(in_ref[:, rows:])
        new_taps_ref[...] = taps_ref[...] + small[:tap_count]
        new_bias_ref[...] = bias_ref[...] + small[tap_count]

    return pl.pallas_call(
        body,
        in_specs=[VMEM] * 4,
        out_shape=[
            jax.ShapeDtypeStruct(sum_w.shape, jnp.float32),
            jax.ShapeDtypeStruct(sum_taps.shape, jnp.float32),
            jax.ShapeDtypeStruct(sum_bias.shape, jnp.float32),
        ],
        cost_estimate=cost(2 * arrived.size, 4 * arrived.size),
        name="last_sum",
        compiler_params=pltpu.CompilerParams(vmem_limit_bytes=24 * 2**20),
    )(near(arrived), near(sum_w), near(sum_taps), near(sum_bias))


def per_device(
    x_next,
    value_next,
    x_prev,
    value_prev,
    cotangent,
    w_gate,
    conv_taps,
    conv_bias,
    sum_w,
    sum_taps,
    sum_bias,
):
    row_count, width = x_next.shape
    n_zh, n_x, n_c = (lax.axis_size(a) for a in ("zh", "x", "c"))
    n_far, n_near = lax.axis_size(FAR), lax.axis_size(NEAR)

    plane = copies_to(copies_to(w_gate, FAR, n_far), NEAR, n_near)
    grad_scale = float(row_count * n_zh * n_far * n_near) ** (-0.5)
    grad_value, gathered, keep, to_core, grad_up, small = previous_branch(
        x_prev, plane, cotangent, value_prev, conv_taps, conv_bias, n_c
    )
    from_core = send_on(to_core, "c", 1)
    sent = weight_gradient(x_prev, grad_up, small, grad_scale, n_near, n_far)
    sent, keep, x_next = lax.optimization_barrier((sent, keep, x_next))
    from_near = exchange(sent, NEAR)

    block_rows = row_count // (n_x * n_c)
    kept = lax.dot_general(
        keep, gathered, (((1,), (1,)), ((), ())), preferred_element_type=jnp.float32
    )
    half = (kept + from_core.astype(jnp.float32)).astype(jnp.bfloat16)
    half = half.reshape(n_x, block_rows, width)
    arrived = [half[0]] + [send_on(half[k], "x", k) for k in range(1, n_x)]
    hidden_next = next_branch(x_next, gathered, value_next, conv_taps, conv_bias)
    from_near, hidden_next, *arrived = lax.optimization_barrier((from_near, hidden_next, *arrived))
    eighth = sum(block.astype(jnp.float32) for block in arrived).astype(jnp.bfloat16)
    spread = [eighth]
    for k in range(1, n_x):
        spread.append(send_on(eighth, "x", k))
    half = jnp.stack(spread)
    grad_input = put_in_order(half, send_on(half, "c", 1), n_c).reshape(row_count, width)

    by_far = sum_and_repack(from_near, n_far, n_zh)
    from_far = exchange(by_far, ("zh", *FAR))
    from_far, grad_input = lax.optimization_barrier((from_far, grad_input))
    new_w, new_taps, new_bias = last_sum(from_far, sum_w, sum_taps, sum_bias)
    return hidden_next, grad_input, grad_value, new_w, new_taps, new_bias


def solution(mesh):
    n_fs, n_tp = mesh.shape["fs"], mesh.shape["tp"]
    n_y, n_c = 4, 2
    n_z = n_fs // n_y
    fine = Mesh(
        mesh.devices.reshape(mesh.shape["rep"], n_z // 4, 2, 2, n_y, n_tp // n_c, n_c),
        ("zh", *FAR, *NEAR, "x", "c"),
    )
    fs, tp = (*FAR, *NEAR), ("x", "c")
    tokens = ("zh", *fs)
    in_specs = (
        P(tokens, None),
        P(tokens, tp),
        P(tokens, None),
        P(tokens, tp),
        P(tokens, tp),
        P(fs, tp),
        P(None, tp),
        P(tp),
        P(fs, tp),
        P(None, tp),
        P(tp),
    )
    out_specs = (
        P(tokens, tp),
        P(tokens, None),
        P(tokens, tp),
        P(fs, tp),
        P(None, tp),
        P(tp),
    )
    return jax.shard_map(
        per_device, mesh=fine, in_specs=in_specs, out_specs=out_specs, check_vma=False
    )
```

```python
import jax
import jax.numpy as jnp
from jax import lax
from jax.experimental import pallas as pl
from jax.experimental.pallas import tpu as pltpu
from jax.sharding import Mesh
from jax.sharding import PartitionSpec as P


SEQ_LEN = 128
SMALL_ROWS = 8
FAR, NEAR = ("zm", "zp"), ("zl", "y")


def copies_to(block, axis, size):
    copies = jnp.broadcast_to(block, (size, *block.shape))
    return lax.all_to_all(copies, axis, 0, 0, tiled=True)


def exchange(blocks, axis):
    return lax.all_to_all(blocks, axis, 0, 0, tiled=True)


def send_on(block, axis, shift):
    size = lax.axis_size(axis)
    return lax.ppermute(block, axis, [(i, (i + shift) % size) for i in range(size)])


def near(array):
    return pltpu.with_memory_space_constraint(array, pltpu.VMEM)


VMEM = pl.BlockSpec(memory_space=pltpu.VMEM)
HBM = pl.BlockSpec(memory_space=pltpu.HBM)


def cost(flops, count, exps=0):
    return pl.CostEstimate(flops=flops, bytes_accessed=count, transcendentals=exps)


def put_in_order(own, other, n_c):
    n_x = own.shape[0]

    def body(own_ref, other_ref, out_ref):
        at_x, at_c = lax.axis_index("x"), lax.axis_index("c")
        for k in range(n_x):
            spot = (at_x + n_x - k) % n_x
            out_ref[at_c * n_x + spot] = own_ref[k]
            out_ref[(1 - at_c) * n_x + spot] = other_ref[k]

    return pl.pallas_call(
        body,
        in_specs=[VMEM] * 2,
        out_shape=jax.ShapeDtypeStruct((n_c * n_x, *own.shape[1:]), own.dtype),
        cost_estimate=cost(0, 8 * own.size),
        name="put_in_order",
        compiler_params=pltpu.CompilerParams(vmem_limit_bytes=24 * 2**20),
    )(near(own), near(other))


def later(values, offset):
    if offset == 0:
        return values
    rows = lax.broadcasted_iota(jnp.int32, values.shape, 0) % SEQ_LEN
    return jnp.where(rows >= offset, pltpu.roll(values, offset, 0), 0.0)


def earlier(values, offset):
    if offset == 0:
        return values
    count = values.shape[0]
    rows = lax.broadcasted_iota(jnp.int32, values.shape, 0) % SEQ_LEN
    return jnp.where(rows < SEQ_LEN - offset, pltpu.roll(values, count - offset, 0), 0.0)


def gated(up, taps_ref, bias_ref):
    tap_count = taps_ref.shape[0]
    total = bias_ref[...][None, :]
    for j in range(tap_count):
        total = total + taps_ref[j : j + 1, :] * later(up, tap_count - 1 - j)
    return total


def high_and_low(rows):
    high = rows.astype(jnp.bfloat16).astype(jnp.float32)
    half = SMALL_ROWS // 2
    return (high + pltpu.roll(rows - high, half, 0)).astype(jnp.bfloat16)


def previous_branch(x_prev, plane, cotangent, value_prev, conv_taps, conv_bias, grad_scale, n_c):
    row_count, width = x_prev.shape
    n_near, n_far, shard_rows, units = plane.shape
    tap_count = conv_taps.shape[0]
    n_x = lax.axis_size("x")
    half_rows = row_count // n_c
    block_rows = half_rows // n_x
    each = n_far * shard_rows

    def body(
        x_ref,
        w_ref,
        cot_ref,
        value_ref,
        taps_ref,
        bias_ref,
        gv_ref,
        natural_ref,
        keep_ref,
        send_out,
        sent_out,
        gu_ref,
        turned_ref,
        send_ref,
        sent_ref,
        sems,
    ):
        spots = [
            (near_at, far_at, (far_at * n_near + near_at) * shard_rows)
            for near_at in range(n_near)
            for far_at in range(n_far)
        ]
        for near_at, far_at, at in spots:
            natural_ref[at : at + shard_rows] = w_ref[near_at, far_at]
        up = jnp.dot(x_ref[...], natural_ref[...], preferred_element_type=jnp.float32)
        up = up.astype(jnp.bfloat16).astype(jnp.float32)
        gate = gated(up, taps_ref, bias_ref)
        sig = jax.nn.sigmoid(gate)
        cot = cot_ref[...].astype(jnp.float32)
        gv_ref[...] = (cot * gate * sig).astype(jnp.bfloat16)
        grad_gate = cot * value_ref[...].astype(jnp.float32) * sig * (1.0 + gate * (1.0 - sig))
        grad_up = jnp.zeros_like(grad_gate)
        for j in range(tap_count):
            grad_up = grad_up + taps_ref[j : j + 1, :] * earlier(grad_gate, tap_count - 1 - j)
        gu_ref[...] = grad_up.astype(jnp.bfloat16)

        at_x, at_c = lax.axis_index("x"), lax.axis_index("c")
        for i, half_ref in ((1, turned_ref), (0, keep_ref)):
            core = (at_c + i) % n_c
            for k in range(n_x):
                row = core * half_rows + ((at_x + k) % n_x) * block_rows
                half_ref[k * block_rows : (k + 1) * block_rows] = gu_ref[
                    pl.ds(pl.multiple_of(row, block_rows), block_rows)
                ]
        send_ref[...] = lax.dot_general(
            turned_ref[...],
            natural_ref[...],
            (((1,), (1,)), ((), ())),
            preferred_element_type=jnp.float32,
        ).astype(jnp.bfloat16)
        moves = [pltpu.make_async_copy(send_ref, send_out, sems.at[n_near])]
        moves[0].start()

        grad_w = lax.dot_general(
            x_ref[...], gu_ref[...], (((0,), (0,)), ((), ())), preferred_element_type=jnp.float32
        )
        grad_w = (grad_w * grad_scale).astype(jnp.bfloat16)
        sums = [
            jnp.sum(grad_gate * later(up, tap_count - 1 - j), axis=0, keepdims=True)
            for j in range(tap_count)
        ] + [jnp.sum(grad_gate, axis=0, keepdims=True)]
        rest = jnp.zeros((SMALL_ROWS - len(sums), units), jnp.float32)
        small = high_and_low(jnp.concatenate([*sums, rest], axis=0) * grad_scale)
        for block in range(n_near):
            for near_at, far_at, at in spots:
                if near_at == block:
                    to = far_at * shard_rows
                    sent_ref[block, to : to + shard_rows] = grad_w[at : at + shard_rows]
            sent_ref[block, each:] = small
            moves.append(
                pltpu.make_async_copy(sent_ref.at[block], sent_out.at[block], sems.at[block])
            )
            moves[-1].start()
        for move in moves:
            move.wait()

    half = jnp.bfloat16
    return pl.pallas_call(
        body,
        in_specs=[VMEM] * 6,
        out_specs=[pl.BlockSpec(), VMEM, VMEM, HBM, HBM],
        out_shape=[
            jax.ShapeDtypeStruct((row_count, units), half),
            pltpu.VMEM((width, units), half),
            pltpu.VMEM((half_rows, units), half),
            pltpu.HBM((half_rows, width), half),
            pltpu.HBM((n_near, each + SMALL_ROWS, units), half),
        ],
        scratch_shapes=[
            pltpu.VMEM((row_count, units), half),
            pltpu.VMEM((half_rows, units), half),
            pltpu.VMEM((half_rows, width), half),
            pltpu.VMEM((n_near, each + SMALL_ROWS, units), half),
            pltpu.SemaphoreType.DMA((n_near + 1,)),
        ],
        cost_estimate=cost(5 * row_count * width * units, 8 * width * units, row_count * units),
        name="previous_branch",
        compiler_params=pltpu.CompilerParams(vmem_limit_bytes=24 * 2**20),
    )(
        near(x_prev),
        near(plane),
        near(cotangent),
        near(value_prev),
        near(conv_taps),
        near(conv_bias),
    )


def next_branch(x_next, weights, value_next, conv_taps, conv_bias):
    row_count, width = x_next.shape
    units = weights.shape[1]

    def body(x_ref, w_ref, value_ref, taps_ref, bias_ref, out_ref):
        up = jnp.dot(x_ref[...], w_ref[...], preferred_element_type=jnp.float32)
        gate = gated(up.astype(jnp.bfloat16).astype(jnp.float32), taps_ref, bias_ref)
        hidden = gate * jax.nn.sigmoid(gate) * value_ref[...].astype(jnp.float32)
        out_ref[...] = hidden.astype(jnp.bfloat16)

    return pl.pallas_call(
        body,
        in_specs=[VMEM] * 5,
        out_shape=jax.ShapeDtypeStruct((row_count, units), jnp.bfloat16),
        cost_estimate=cost(2 * row_count * width * units, 4 * width * units, row_count * units),
        name="next_branch",
        compiler_params=pltpu.CompilerParams(vmem_limit_bytes=24 * 2**20),
    )(near(x_next), near(weights), near(value_next), near(conv_taps), near(conv_bias))


def summed(block):
    return jnp.sum(block.astype(jnp.float32), axis=0)


def small_total(block):
    total = summed(block)
    half = SMALL_ROWS // 2
    rows = lax.broadcasted_iota(jnp.int32, total.shape, 0)
    return jnp.where(rows < half, total + pltpu.roll(total, half, 0), 0.0)


def sum_and_repack(arrived, parts, repeats):
    _, rows, units = arrived.shape
    extra = SMALL_ROWS
    each = (rows - extra) // parts

    def body(in_ref, out_ref, block_ref, sems):
        small = high_and_low(small_total(in_ref[:, rows - extra :]))
        moves = []
        for p in range(parts):
            main = summed(in_ref[:, p * each : (p + 1) * each]).astype(jnp.bfloat16)
            block_ref[p, :each] = main
            block_ref[p, each:] = small
            for r in range(repeats):
                to = r * parts + p
                move = pltpu.make_async_copy(block_ref.at[p], out_ref.at[to], sems.at[to])
                move.start()
                moves.append(move)
        for move in moves:
            move.wait()

    return pl.pallas_call(
        body,
        in_specs=[VMEM],
        out_specs=HBM,
        out_shape=pltpu.HBM((repeats * parts, each + extra, units), jnp.bfloat16),
        scratch_shapes=[
            pltpu.VMEM((parts, each + extra, units), jnp.bfloat16),
            pltpu.SemaphoreType.DMA((repeats * parts,)),
        ],
        cost_estimate=cost(2 * arrived.size, 4 * arrived.size),
        name="sum_and_repack",
        compiler_params=pltpu.CompilerParams(vmem_limit_bytes=24 * 2**20),
    )(near(arrived))


def last_sum(arrived, sum_w, sum_taps, sum_bias):
    rows, _ = sum_w.shape
    tap_count = sum_taps.shape[0]

    def body(in_ref, w_ref, taps_ref, bias_ref, new_w_ref, new_taps_ref, new_bias_ref):
        new_w_ref[...] = w_ref[...] + summed(in_ref[:, :rows])
        small = small_total(in_ref[:, rows:])
        new_taps_ref[...] = taps_ref[...] + small[:tap_count]
        new_bias_ref[...] = bias_ref[...] + small[tap_count]

    return pl.pallas_call(
        body,
        in_specs=[VMEM] * 4,
        out_shape=[
            jax.ShapeDtypeStruct(sum_w.shape, jnp.float32),
            jax.ShapeDtypeStruct(sum_taps.shape, jnp.float32),
            jax.ShapeDtypeStruct(sum_bias.shape, jnp.float32),
        ],
        cost_estimate=cost(2 * arrived.size, 4 * arrived.size),
        name="last_sum",
        compiler_params=pltpu.CompilerParams(vmem_limit_bytes=24 * 2**20),
    )(near(arrived), near(sum_w), near(sum_taps), near(sum_bias))


def per_device(
    x_next,
    value_next,
    x_prev,
    value_prev,
    cotangent,
    w_gate,
    conv_taps,
    conv_bias,
    sum_w,
    sum_taps,
    sum_bias,
):
    row_count, width = x_next.shape
    n_zh, n_x, n_c = (lax.axis_size(a) for a in ("zh", "x", "c"))
    n_far, n_near = lax.axis_size(FAR), lax.axis_size(NEAR)

    plane = copies_to(copies_to(w_gate, FAR, n_far), NEAR, n_near)
    grad_scale = float(row_count * n_zh * n_far * n_near) ** (-0.5)
    grad_value, gathered, keep, to_core, sent = previous_branch(
        x_prev, plane, cotangent, value_prev, conv_taps, conv_bias, grad_scale, n_c
    )
    from_core = send_on(to_core, "c", 1)
    from_near = exchange(sent, NEAR)

    block_rows = row_count // (n_x * n_c)
    kept = lax.dot_general(
        keep, gathered, (((1,), (1,)), ((), ())), preferred_element_type=jnp.float32
    )
    half = (kept + from_core.astype(jnp.float32)).astype(jnp.bfloat16)
    half = half.reshape(n_x, block_rows, width)
    arrived = [half[0]]
    for k in range(1, n_x):
        arrived.append(send_on(half[k], "x", k))
    hidden_next = next_branch(x_next, gathered, value_next, conv_taps, conv_bias)
    from_near, hidden_next = lax.optimization_barrier((from_near, hidden_next))
    by_far = sum_and_repack(from_near, n_far, n_zh)
    from_far = exchange(by_far, ("zh", *FAR))

    eighth = sum(block.astype(jnp.float32) for block in arrived).astype(jnp.bfloat16)
    half = jnp.stack([eighth] + [send_on(eighth, "x", k) for k in range(1, n_x)])
    grad_input = put_in_order(half, send_on(half, "c", 1), n_c).reshape(row_count, width)
    from_far, grad_input = lax.optimization_barrier((from_far, grad_input))
    new_w, new_taps, new_bias = last_sum(from_far, sum_w, sum_taps, sum_bias)
    return hidden_next, grad_input, grad_value, new_w, new_taps, new_bias


def solution(mesh):
    n_fs, n_tp = mesh.shape["fs"], mesh.shape["tp"]
    n_y, n_c = 4, 2
    n_z = n_fs // n_y
    fine = Mesh(
        mesh.devices.reshape(mesh.shape["rep"], n_z // 4, 2, 2, n_y, n_tp // n_c, n_c),
        ("zh", *FAR, *NEAR, "x", "c"),
    )
    fs, tp = (*FAR, *NEAR), ("x", "c")
    tokens = ("zh", *fs)
    in_specs = (
        P(tokens, None),
        P(tokens, tp),
        P(tokens, None),
        P(tokens, tp),
        P(tokens, tp),
        P(fs, tp),
        P(None, tp),
        P(tp),
        P(fs, tp),
        P(None, tp),
        P(tp),
    )
    out_specs = (
        P(tokens, tp),
        P(tokens, None),
        P(tokens, tp),
        P(fs, tp),
        P(None, tp),
        P(tp),
    )
    return jax.shard_map(
        per_device, mesh=fine, in_specs=in_specs, out_specs=out_specs, check_vma=False
    )
```

```python
import jax
import jax.numpy as jnp
from jax import lax
from jax.experimental import pallas as pl
from jax.experimental.pallas import tpu as pltpu
from jax.sharding import Mesh
from jax.sharding import PartitionSpec as P


SEQ_LEN = 128
SMALL_ROWS = 8
FAR, NEAR = ("zm", "zp"), ("zl", "y")


def copies_to(block, axis, size):
    copies = jnp.broadcast_to(block, (size, *block.shape))
    return lax.all_to_all(copies, axis, 0, 0, tiled=True)


def exchange(blocks, axis):
    return lax.all_to_all(blocks, axis, 0, 0, tiled=True)


def send_on(block, axis, shift):
    size = lax.axis_size(axis)
    return lax.ppermute(block, axis, [(i, (i + shift) % size) for i in range(size)])


def near(array):
    return pltpu.with_memory_space_constraint(array, pltpu.VMEM)


VMEM = pl.BlockSpec(memory_space=pltpu.VMEM)
HBM = pl.BlockSpec(memory_space=pltpu.HBM)


def cost(flops, count, exps=0):
    return pl.CostEstimate(flops=flops, bytes_accessed=count, transcendentals=exps)


def put_in_order(own, other, n_c):
    n_x = own.shape[0]

    def body(own_ref, other_ref, out_ref):
        at_x, at_c = lax.axis_index("x"), lax.axis_index("c")
        for k in range(n_x):
            spot = (at_x + n_x - k) % n_x
            out_ref[at_c * n_x + spot] = own_ref[k]
            out_ref[(1 - at_c) * n_x + spot] = other_ref[k]

    return pl.pallas_call(
        body,
        in_specs=[VMEM] * 2,
        out_shape=jax.ShapeDtypeStruct((n_c * n_x, *own.shape[1:]), own.dtype),
        cost_estimate=cost(0, 8 * own.size),
        name="put_in_order",
        compiler_params=pltpu.CompilerParams(vmem_limit_bytes=24 * 2**20),
    )(near(own), near(other))


def later(values, offset):
    if offset == 0:
        return values
    rows = lax.broadcasted_iota(jnp.int32, values.shape, 0) % SEQ_LEN
    return jnp.where(rows >= offset, pltpu.roll(values, offset, 0), 0.0)


def earlier(values, offset):
    if offset == 0:
        return values
    count = values.shape[0]
    rows = lax.broadcasted_iota(jnp.int32, values.shape, 0) % SEQ_LEN
    return jnp.where(rows < SEQ_LEN - offset, pltpu.roll(values, count - offset, 0), 0.0)


def gated(up, taps_ref, bias_ref):
    tap_count = taps_ref.shape[0]
    total = bias_ref[...][None, :]
    for j in range(tap_count):
        total = total + taps_ref[j : j + 1, :] * later(up, tap_count - 1 - j)
    return total


def high_and_low(rows):
    high = rows.astype(jnp.bfloat16).astype(jnp.float32)
    half = SMALL_ROWS // 2
    return (high + pltpu.roll(rows - high, half, 0)).astype(jnp.bfloat16)


def previous_branch(x_prev, plane, cotangent, value_prev, conv_taps, conv_bias, grad_scale, n_c):
    row_count, width = x_prev.shape
    n_near, n_far, shard_rows, units = plane.shape
    tap_count = conv_taps.shape[0]
    n_x = lax.axis_size("x")
    half_rows = row_count // n_c
    block_rows = half_rows // n_x
    each = n_far * shard_rows

    def body(
        x_ref,
        w_ref,
        cot_ref,
        value_ref,
        taps_ref,
        bias_ref,
        gv_ref,
        natural_ref,
        keep_ref,
        send_out,
        sent_out,
        gu_ref,
        turned_ref,
        send_ref,
        sent_ref,
        sems,
    ):
        spots = [
            (near_at, far_at, (far_at * n_near + near_at) * shard_rows)
            for near_at in range(n_near)
            for far_at in range(n_far)
        ]
        for near_at, far_at, at in spots:
            natural_ref[at : at + shard_rows] = w_ref[near_at, far_at]
        up = jnp.dot(x_ref[...], natural_ref[...], preferred_element_type=jnp.float32)
        up = up.astype(jnp.bfloat16).astype(jnp.float32)
        gate = gated(up, taps_ref, bias_ref)
        sig = jax.nn.sigmoid(gate)
        cot = cot_ref[...].astype(jnp.float32)
        gv_ref[...] = (cot * gate * sig).astype(jnp.bfloat16)
        grad_gate = cot * value_ref[...].astype(jnp.float32) * sig * (1.0 + gate * (1.0 - sig))
        grad_up = jnp.zeros_like(grad_gate)
        for j in range(tap_count):
            grad_up = grad_up + taps_ref[j : j + 1, :] * earlier(grad_gate, tap_count - 1 - j)
        gu_ref[...] = grad_up.astype(jnp.bfloat16)

        at_x, at_c = lax.axis_index("x"), lax.axis_index("c")
        for i, half_ref in ((1, turned_ref), (0, keep_ref)):
            core = (at_c + i) % n_c
            for k in range(n_x):
                row = core * half_rows + ((at_x + k) % n_x) * block_rows
                half_ref[k * block_rows : (k + 1) * block_rows] = gu_ref[
                    pl.ds(pl.multiple_of(row, block_rows), block_rows)
                ]
        send_ref[...] = lax.dot_general(
            turned_ref[...],
            natural_ref[...],
            (((1,), (1,)), ((), ())),
            preferred_element_type=jnp.float32,
        ).astype(jnp.bfloat16)
        moves = [pltpu.make_async_copy(send_ref, send_out, sems.at[n_near])]
        moves[0].start()

        grad_w = lax.dot_general(
            x_ref[...], gu_ref[...], (((0,), (0,)), ((), ())), preferred_element_type=jnp.float32
        )
        grad_w = (grad_w * grad_scale).astype(jnp.bfloat16)
        sums = [
            jnp.sum(grad_gate * later(up, tap_count - 1 - j), axis=0, keepdims=True)
            for j in range(tap_count)
        ] + [jnp.sum(grad_gate, axis=0, keepdims=True)]
        rest = jnp.zeros((SMALL_ROWS - len(sums), units), jnp.float32)
        small = high_and_low(jnp.concatenate([*sums, rest], axis=0) * grad_scale)
        for block in range(n_near):
            for near_at, far_at, at in spots:
                if near_at == block:
                    to = far_at * shard_rows
                    sent_ref[block, to : to + shard_rows] = grad_w[at : at + shard_rows]
            sent_ref[block, each:] = small
            moves.append(
                pltpu.make_async_copy(sent_ref.at[block], sent_out.at[block], sems.at[block])
            )
            moves[-1].start()
        for move in moves:
            move.wait()

    half = jnp.bfloat16
    return pl.pallas_call(
        body,
        in_specs=[VMEM] * 6,
        out_specs=[pl.BlockSpec(), VMEM, VMEM, HBM, HBM],
        out_shape=[
            jax.ShapeDtypeStruct((row_count, units), half),
            pltpu.VMEM((width, units), half),
            pltpu.VMEM((half_rows, units), half),
            pltpu.HBM((half_rows, width), half),
            pltpu.HBM((n_near, each + SMALL_ROWS, units), half),
        ],
        scratch_shapes=[
            pltpu.VMEM((row_count, units), half),
            pltpu.VMEM((half_rows, units), half),
            pltpu.VMEM((half_rows, width), half),
            pltpu.VMEM((n_near, each + SMALL_ROWS, units), half),
            pltpu.SemaphoreType.DMA((n_near + 1,)),
        ],
        cost_estimate=cost(5 * row_count * width * units, 8 * width * units, row_count * units),
        name="previous_branch",
        compiler_params=pltpu.CompilerParams(vmem_limit_bytes=24 * 2**20),
    )(
        near(x_prev),
        near(plane),
        near(cotangent),
        near(value_prev),
        near(conv_taps),
        near(conv_bias),
    )


def add_halves(keep, weights, from_core, n_x):
    rows, width = from_core.shape
    each = rows // n_x

    def body(keep_ref, w_ref, other_ref, *refs):
        out_refs, blocks_ref, sems = refs[:n_x], refs[n_x], refs[n_x + 1]
        total = lax.dot_general(
            keep_ref[...],
            w_ref[...],
            (((1,), (1,)), ((), ())),
            preferred_element_type=jnp.float32,
        )
        total = (total + other_ref[...].astype(jnp.float32)).astype(jnp.bfloat16)
        moves = []
        for k in range(n_x):
            blocks_ref[k] = total[k * each : (k + 1) * each]
            moves.append(pltpu.make_async_copy(blocks_ref.at[k], out_refs[k], sems.at[k]))
            moves[-1].start()
        for move in moves:
            move.wait()

    return pl.pallas_call(
        body,
        in_specs=[VMEM] * 3,
        out_specs=[HBM] * n_x,
        out_shape=[pltpu.HBM((each, width), jnp.bfloat16)] * n_x,
        scratch_shapes=[
            pltpu.VMEM((n_x, each, width), jnp.bfloat16),
            pltpu.SemaphoreType.DMA((n_x,)),
        ],
        cost_estimate=cost(2 * keep.size * width, 8 * weights.size),
        name="add_halves",
        compiler_params=pltpu.CompilerParams(vmem_limit_bytes=16 * 2**20),
    )(near(keep), near(weights), near(from_core))


def next_branch(x_next, weights, value_next, conv_taps, conv_bias):
    row_count, width = x_next.shape
    units = weights.shape[1]

    def body(x_ref, w_ref, value_ref, taps_ref, bias_ref, out_ref):
        up = jnp.dot(x_ref[...], w_ref[...], preferred_element_type=jnp.float32)
        gate = gated(up.astype(jnp.bfloat16).astype(jnp.float32), taps_ref, bias_ref)
        hidden = gate * jax.nn.sigmoid(gate) * value_ref[...].astype(jnp.float32)
        out_ref[...] = hidden.astype(jnp.bfloat16)

    return pl.pallas_call(
        body,
        in_specs=[VMEM] * 5,
        out_shape=jax.ShapeDtypeStruct((row_count, units), jnp.bfloat16),
        cost_estimate=cost(2 * row_count * width * units, 4 * width * units, row_count * units),
        name="next_branch",
        compiler_params=pltpu.CompilerParams(vmem_limit_bytes=24 * 2**20),
    )(near(x_next), near(weights), near(value_next), near(conv_taps), near(conv_bias))


def summed(block):
    return jnp.sum(block.astype(jnp.float32), axis=0)


def small_total(block):
    total = summed(block)
    half = SMALL_ROWS // 2
    rows = lax.broadcasted_iota(jnp.int32, total.shape, 0)
    return jnp.where(rows < half, total + pltpu.roll(total, half, 0), 0.0)


def sum_and_repack(arrived, parts, repeats):
    _, rows, units = arrived.shape
    extra = SMALL_ROWS
    each = (rows - extra) // parts

    def body(in_ref, out_ref, block_ref, sems):
        small = high_and_low(small_total(in_ref[:, rows - extra :]))
        moves = []
        for p in range(parts):
            main = summed(in_ref[:, p * each : (p + 1) * each]).astype(jnp.bfloat16)
            block_ref[p, :each] = main
            block_ref[p, each:] = small
            for r in range(repeats):
                to = r * parts + p
                move = pltpu.make_async_copy(block_ref.at[p], out_ref.at[to], sems.at[to])
                move.start()
                moves.append(move)
        for move in moves:
            move.wait()

    return pl.pallas_call(
        body,
        in_specs=[VMEM],
        out_specs=HBM,
        out_shape=pltpu.HBM((repeats * parts, each + extra, units), jnp.bfloat16),
        scratch_shapes=[
            pltpu.VMEM((parts, each + extra, units), jnp.bfloat16),
            pltpu.SemaphoreType.DMA((repeats * parts,)),
        ],
        cost_estimate=cost(2 * arrived.size, 4 * arrived.size),
        name="sum_and_repack",
        compiler_params=pltpu.CompilerParams(vmem_limit_bytes=24 * 2**20),
    )(near(arrived))


def last_sum(arrived, sum_w, sum_taps, sum_bias):
    rows, _ = sum_w.shape
    tap_count = sum_taps.shape[0]

    def body(in_ref, w_ref, taps_ref, bias_ref, new_w_ref, new_taps_ref, new_bias_ref):
        new_w_ref[...] = w_ref[...] + summed(in_ref[:, :rows])
        small = small_total(in_ref[:, rows:])
        new_taps_ref[...] = taps_ref[...] + small[:tap_count]
        new_bias_ref[...] = bias_ref[...] + small[tap_count]

    return pl.pallas_call(
        body,
        in_specs=[VMEM] * 4,
        out_shape=[
            jax.ShapeDtypeStruct(sum_w.shape, jnp.float32),
            jax.ShapeDtypeStruct(sum_taps.shape, jnp.float32),
            jax.ShapeDtypeStruct(sum_bias.shape, jnp.float32),
        ],
        cost_estimate=cost(2 * arrived.size, 4 * arrived.size),
        name="last_sum",
        compiler_params=pltpu.CompilerParams(vmem_limit_bytes=24 * 2**20),
    )(near(arrived), near(sum_w), near(sum_taps), near(sum_bias))


def per_device(
    x_next,
    value_next,
    x_prev,
    value_prev,
    cotangent,
    w_gate,
    conv_taps,
    conv_bias,
    sum_w,
    sum_taps,
    sum_bias,
):
    row_count, width = x_next.shape
    n_zh, n_x, n_c = (lax.axis_size(a) for a in ("zh", "x", "c"))
    n_far, n_near = lax.axis_size(FAR), lax.axis_size(NEAR)

    plane = copies_to(copies_to(w_gate, FAR, n_far), NEAR, n_near)
    grad_scale = float(row_count * n_zh * n_far * n_near) ** (-0.5)
    grad_value, gathered, keep, to_core, sent = previous_branch(
        x_prev, plane, cotangent, value_prev, conv_taps, conv_bias, grad_scale, n_c
    )
    from_core = send_on(to_core, "c", 1)
    from_near = exchange(sent, NEAR)

    half = add_halves(keep, gathered, from_core, n_x)
    arrived = [half[0]]
    for k in range(1, n_x):
        arrived.append(send_on(half[k], "x", k))
    by_far = sum_and_repack(from_near, n_far, n_zh)
    from_far = exchange(by_far, ("zh", *FAR))

    eighth = sum(block.astype(jnp.float32) for block in arrived).astype(jnp.bfloat16)
    spread = [eighth]
    for k in range(1, n_x):
        spread.append(send_on(eighth, "x", k))
    eighth, x_next = lax.optimization_barrier((eighth, x_next))
    hidden_next = next_branch(x_next, gathered, value_next, conv_taps, conv_bias)
    hidden_next, *spread = lax.optimization_barrier((hidden_next, *spread))
    half = jnp.stack(spread)
    grad_input = put_in_order(half, send_on(half, "c", 1), n_c).reshape(row_count, width)
    from_far, grad_input = lax.optimization_barrier((from_far, grad_input))
    new_w, new_taps, new_bias = last_sum(from_far, sum_w, sum_taps, sum_bias)
    return hidden_next, grad_input, grad_value, new_w, new_taps, new_bias


def solution(mesh):
    n_fs, n_tp = mesh.shape["fs"], mesh.shape["tp"]
    n_y, n_c = 4, 2
    n_z = n_fs // n_y
    fine = Mesh(
        mesh.devices.reshape(mesh.shape["rep"], n_z // 4, 2, 2, n_y, n_tp // n_c, n_c),
        ("zh", *FAR, *NEAR, "x", "c"),
    )
    fs, tp = (*FAR, *NEAR), ("x", "c")
    tokens = ("zh", *fs)
    in_specs = (
        P(tokens, None),
        P(tokens, tp),
        P(tokens, None),
        P(tokens, tp),
        P(tokens, tp),
        P(fs, tp),
        P(None, tp),
        P(tp),
        P(fs, tp),
        P(None, tp),
        P(tp),
    )
    out_specs = (
        P(tokens, tp),
        P(tokens, None),
        P(tokens, tp),
        P(fs, tp),
        P(None, tp),
        P(tp),
    )
    return jax.shard_map(
        per_device, mesh=fine, in_specs=in_specs, out_specs=out_specs, check_vma=False
    )
```

```python
import jax
import jax.numpy as jnp
from jax import lax
from jax.experimental import pallas as pl
from jax.experimental.pallas import tpu as pltpu
from jax.sharding import Mesh
from jax.sharding import PartitionSpec as P


SEQ_LEN = 128
SMALL_ROWS = 8
FAR, NEAR = ("zm", "zp"), ("zl", "y")


def copies_to(block, axis, size):
    copies = jnp.broadcast_to(block, (size, *block.shape))
    return lax.all_to_all(copies, axis, 0, 0, tiled=True)


def exchange(blocks, axis):
    return lax.all_to_all(blocks, axis, 0, 0, tiled=True)


def send_on(block, axis, shift):
    size = lax.axis_size(axis)
    return lax.ppermute(block, axis, [(i, (i + shift) % size) for i in range(size)])


def near(array):
    return pltpu.with_memory_space_constraint(array, pltpu.VMEM)


VMEM = pl.BlockSpec(memory_space=pltpu.VMEM)
HBM = pl.BlockSpec(memory_space=pltpu.HBM)


def cost(flops, count, exps=0):
    return pl.CostEstimate(flops=flops, bytes_accessed=count, transcendentals=exps)


def put_in_order(own, other, n_c):
    n_x = own.shape[0]

    def body(own_ref, other_ref, out_ref):
        at_x, at_c = lax.axis_index("x"), lax.axis_index("c")
        for k in range(n_x):
            spot = (at_x + n_x - k) % n_x
            out_ref[at_c * n_x + spot] = own_ref[k]
            out_ref[(1 - at_c) * n_x + spot] = other_ref[k]

    return pl.pallas_call(
        body,
        in_specs=[VMEM] * 2,
        out_shape=jax.ShapeDtypeStruct((n_c * n_x, *own.shape[1:]), own.dtype),
        cost_estimate=cost(0, 8 * own.size),
        name="put_in_order",
        compiler_params=pltpu.CompilerParams(vmem_limit_bytes=24 * 2**20),
    )(near(own), near(other))


EDGE = 8


def later(values, offset):
    if offset == 0:
        return values
    moved = pltpu.roll(values, offset, 0)
    pieces = []
    for start in range(0, values.shape[0], SEQ_LEN):
        edge = moved[start : start + EDGE]
        rows = lax.broadcasted_iota(jnp.int32, edge.shape, 0)
        pieces.append(jnp.where(rows >= offset, edge, 0.0))
        pieces.append(moved[start + EDGE : start + SEQ_LEN])
    return jnp.concatenate(pieces, axis=0)


def earlier(values, offset):
    if offset == 0:
        return values
    moved = pltpu.roll(values, values.shape[0] - offset, 0)
    pieces = []
    for end in range(SEQ_LEN, values.shape[0] + 1, SEQ_LEN):
        pieces.append(moved[end - SEQ_LEN : end - EDGE])
        edge = moved[end - EDGE : end]
        rows = lax.broadcasted_iota(jnp.int32, edge.shape, 0)
        pieces.append(jnp.where(rows < EDGE - offset, edge, 0.0))
    return jnp.concatenate(pieces, axis=0)


def lags_of(up, tap_count):
    return [later(up, tap_count - 1 - j) for j in range(tap_count)]


def gated(lags, taps_ref, bias_ref):
    total = bias_ref[...][None, :]
    for j, lag in enumerate(lags):
        total = total + taps_ref[j : j + 1, :] * lag
    return total


def high_and_low(rows):
    high = rows.astype(jnp.bfloat16).astype(jnp.float32)
    half = SMALL_ROWS // 2
    return (high + pltpu.roll(rows - high, half, 0)).astype(jnp.bfloat16)


def previous_branch(x_prev, plane, cotangent, value_prev, conv_taps, conv_bias, grad_scale):
    row_count, width = x_prev.shape
    n_near, n_far, shard_rows, units = plane.shape
    tap_count = conv_taps.shape[0]
    each = n_far * shard_rows

    def body(
        x_ref,
        w_ref,
        cot_ref,
        value_ref,
        taps_ref,
        bias_ref,
        gv_ref,
        natural_ref,
        gu_ref,
        sent_out,
        sent_ref,
        sems,
    ):
        spots = [
            (near_at, far_at, (far_at * n_near + near_at) * shard_rows)
            for near_at in range(n_near)
            for far_at in range(n_far)
        ]
        for near_at, far_at, at in spots:
            natural_ref[at : at + shard_rows] = w_ref[near_at, far_at]
        up = jnp.dot(x_ref[...], natural_ref[...], preferred_element_type=jnp.float32)
        up = up.astype(jnp.bfloat16).astype(jnp.float32)
        lags = lags_of(up, tap_count)
        gate = gated(lags, taps_ref, bias_ref)
        sig = jax.nn.sigmoid(gate)
        cot = cot_ref[...].astype(jnp.float32)
        gv_ref[...] = (cot * gate * sig).astype(jnp.bfloat16)
        grad_gate = cot * value_ref[...].astype(jnp.float32) * sig * (1.0 + gate * (1.0 - sig))
        grad_up = jnp.zeros_like(grad_gate)
        for j in range(tap_count):
            grad_up = grad_up + taps_ref[j : j + 1, :] * earlier(grad_gate, tap_count - 1 - j)
        gu_ref[...] = grad_up.astype(jnp.bfloat16)

        grad_w = lax.dot_general(
            x_ref[...], gu_ref[...], (((0,), (0,)), ((), ())), preferred_element_type=jnp.float32
        )
        grad_w = (grad_w * grad_scale).astype(jnp.bfloat16)
        sums = [
            jnp.sum(grad_gate * lag, axis=0, keepdims=True) for lag in lags
        ] + [jnp.sum(grad_gate, axis=0, keepdims=True)]
        rest = jnp.zeros((SMALL_ROWS - len(sums), units), jnp.float32)
        small = high_and_low(jnp.concatenate([*sums, rest], axis=0) * grad_scale)
        moves = []
        for block in range(n_near):
            for near_at, far_at, at in spots:
                if near_at == block:
                    to = far_at * shard_rows
                    sent_ref[block, to : to + shard_rows] = grad_w[at : at + shard_rows]
            sent_ref[block, each:] = small
            moves.append(
                pltpu.make_async_copy(sent_ref.at[block], sent_out.at[block], sems.at[block])
            )
            moves[-1].start()
        for move in moves:
            move.wait()

    half = jnp.bfloat16
    return pl.pallas_call(
        body,
        in_specs=[VMEM] * 6,
        out_specs=[pl.BlockSpec(), VMEM, VMEM, HBM],
        out_shape=[
            jax.ShapeDtypeStruct((row_count, units), half),
            pltpu.VMEM((width, units), half),
            pltpu.VMEM((row_count, units), half),
            pltpu.HBM((n_near, each + SMALL_ROWS, units), half),
        ],
        scratch_shapes=[
            pltpu.VMEM((n_near, each + SMALL_ROWS, units), half),
            pltpu.SemaphoreType.DMA((n_near,)),
        ],
        cost_estimate=cost(4 * row_count * width * units, 8 * width * units, row_count * units),
        name="previous_branch",
        compiler_params=pltpu.CompilerParams(vmem_limit_bytes=24 * 2**20),
    )(
        near(x_prev),
        near(plane),
        near(cotangent),
        near(value_prev),
        near(conv_taps),
        near(conv_bias),
    )


def core_halves(grad_up, weights, n_c, n_x):
    row_count, units = grad_up.shape
    width = weights.shape[0]
    half_rows = row_count // n_c
    block_rows = half_rows // n_x

    def body(gu_ref, natural_ref, keep_ref, send_out, turned_ref, send_ref, sem):
        at_x, at_c = lax.axis_index("x"), lax.axis_index("c")
        for i, half_ref in ((1, turned_ref), (0, keep_ref)):
            core = (at_c + i) % n_c
            for k in range(n_x):
                row = core * half_rows + ((at_x + k) % n_x) * block_rows
                half_ref[k * block_rows : (k + 1) * block_rows] = gu_ref[
                    pl.ds(pl.multiple_of(row, block_rows), block_rows)
                ]
        send_ref[...] = lax.dot_general(
            turned_ref[...],
            natural_ref[...],
            (((1,), (1,)), ((), ())),
            preferred_element_type=jnp.float32,
        ).astype(jnp.bfloat16)
        move = pltpu.make_async_copy(send_ref, send_out, sem)
        move.start()
        move.wait()

    half = jnp.bfloat16
    return pl.pallas_call(
        body,
        in_specs=[VMEM] * 2,
        out_specs=[VMEM, HBM],
        out_shape=[pltpu.VMEM((half_rows, units), half), pltpu.HBM((half_rows, width), half)],
        scratch_shapes=[
            pltpu.VMEM((half_rows, units), half),
            pltpu.VMEM((half_rows, width), half),
            pltpu.SemaphoreType.DMA(()),
        ],
        cost_estimate=cost(row_count * width * units, 4 * width * units),
        name="core_halves",
        compiler_params=pltpu.CompilerParams(vmem_limit_bytes=16 * 2**20),
    )(near(grad_up), near(weights))


def add_halves(keep, weights, from_core, n_x):
    rows, width = from_core.shape
    each = rows // n_x

    def body(keep_ref, w_ref, other_ref, *refs):
        out_refs, blocks_ref, sems = refs[:n_x], refs[n_x], refs[n_x + 1]
        total = lax.dot_general(
            keep_ref[...],
            w_ref[...],
            (((1,), (1,)), ((), ())),
            preferred_element_type=jnp.float32,
        )
        total = (total + other_ref[...].astype(jnp.float32)).astype(jnp.bfloat16)
        moves = []
        for k in range(n_x):
            blocks_ref[k] = total[k * each : (k + 1) * each]
            moves.append(pltpu.make_async_copy(blocks_ref.at[k], out_refs[k], sems.at[k]))
            moves[-1].start()
        for move in moves:
            move.wait()

    return pl.pallas_call(
        body,
        in_specs=[VMEM] * 3,
        out_specs=[HBM] * n_x,
        out_shape=[pltpu.HBM((each, width), jnp.bfloat16)] * n_x,
        scratch_shapes=[
            pltpu.VMEM((n_x, each, width), jnp.bfloat16),
            pltpu.SemaphoreType.DMA((n_x,)),
        ],
        cost_estimate=cost(2 * keep.size * width, 8 * weights.size),
        name="add_halves",
        compiler_params=pltpu.CompilerParams(vmem_limit_bytes=16 * 2**20),
    )(near(keep), near(weights), near(from_core))


def next_branch(x_next, weights, value_next, conv_taps, conv_bias):
    row_count, width = x_next.shape
    units = weights.shape[1]

    def body(x_ref, w_ref, value_ref, taps_ref, bias_ref, out_ref):
        up = jnp.dot(x_ref[...], w_ref[...], preferred_element_type=jnp.float32)
        up = up.astype(jnp.bfloat16).astype(jnp.float32)
        gate = gated(lags_of(up, taps_ref.shape[0]), taps_ref, bias_ref)
        hidden = gate * jax.nn.sigmoid(gate) * value_ref[...].astype(jnp.float32)
        out_ref[...] = hidden.astype(jnp.bfloat16)

    return pl.pallas_call(
        body,
        in_specs=[VMEM] * 5,
        out_shape=jax.ShapeDtypeStruct((row_count, units), jnp.bfloat16),
        cost_estimate=cost(2 * row_count * width * units, 4 * width * units, row_count * units),
        name="next_branch",
        compiler_params=pltpu.CompilerParams(vmem_limit_bytes=24 * 2**20),
    )(near(x_next), near(weights), near(value_next), near(conv_taps), near(conv_bias))


def summed(block):
    return jnp.sum(block.astype(jnp.float32), axis=0)


def small_total(block):
    total = summed(block)
    half = SMALL_ROWS // 2
    rows = lax.broadcasted_iota(jnp.int32, total.shape, 0)
    return jnp.where(rows < half, total + pltpu.roll(total, half, 0), 0.0)


def sum_and_repack(arrived, parts, repeats):
    _, rows, units = arrived.shape
    extra = SMALL_ROWS
    each = (rows - extra) // parts

    def body(in_ref, out_ref, block_ref, sems):
        small = high_and_low(small_total(in_ref[:, rows - extra :]))
        moves = []
        for p in range(parts):
            main = summed(in_ref[:, p * each : (p + 1) * each]).astype(jnp.bfloat16)
            block_ref[p, :each] = main
            block_ref[p, each:] = small
            for r in range(repeats):
                to = r * parts + p
                move = pltpu.make_async_copy(block_ref.at[p], out_ref.at[to], sems.at[to])
                move.start()
                moves.append(move)
        for move in moves:
            move.wait()

    return pl.pallas_call(
        body,
        in_specs=[VMEM],
        out_specs=HBM,
        out_shape=pltpu.HBM((repeats * parts, each + extra, units), jnp.bfloat16),
        scratch_shapes=[
            pltpu.VMEM((parts, each + extra, units), jnp.bfloat16),
            pltpu.SemaphoreType.DMA((repeats * parts,)),
        ],
        cost_estimate=cost(2 * arrived.size, 4 * arrived.size),
        name="sum_and_repack",
        compiler_params=pltpu.CompilerParams(vmem_limit_bytes=24 * 2**20),
    )(near(arrived))


def last_sum(arrived, sum_w, sum_taps, sum_bias):
    rows, _ = sum_w.shape
    tap_count = sum_taps.shape[0]

    def body(in_ref, w_ref, taps_ref, bias_ref, new_w_ref, new_taps_ref, new_bias_ref):
        new_w_ref[...] = w_ref[...] + summed(in_ref[:, :rows])
        small = small_total(in_ref[:, rows:])
        new_taps_ref[...] = taps_ref[...] + small[:tap_count]
        new_bias_ref[...] = bias_ref[...] + small[tap_count]

    return pl.pallas_call(
        body,
        in_specs=[VMEM] * 4,
        out_shape=[
            jax.ShapeDtypeStruct(sum_w.shape, jnp.float32),
            jax.ShapeDtypeStruct(sum_taps.shape, jnp.float32),
            jax.ShapeDtypeStruct(sum_bias.shape, jnp.float32),
        ],
        cost_estimate=cost(2 * arrived.size, 4 * arrived.size),
        name="last_sum",
        compiler_params=pltpu.CompilerParams(vmem_limit_bytes=24 * 2**20),
    )(near(arrived), near(sum_w), near(sum_taps), near(sum_bias))


def per_device(
    x_next,
    value_next,
    x_prev,
    value_prev,
    cotangent,
    w_gate,
    conv_taps,
    conv_bias,
    sum_w,
    sum_taps,
    sum_bias,
):
    row_count, width = x_next.shape
    n_zh, n_x, n_c = (lax.axis_size(a) for a in ("zh", "x", "c"))
    n_far, n_near = lax.axis_size(FAR), lax.axis_size(NEAR)

    plane = copies_to(copies_to(w_gate, FAR, n_far), NEAR, n_near)
    grad_scale = float(row_count * n_zh * n_far * n_near) ** (-0.5)
    grad_value, gathered, grad_up, sent = previous_branch(
        x_prev, plane, cotangent, value_prev, conv_taps, conv_bias, grad_scale
    )
    sent, grad_up = lax.optimization_barrier((sent, grad_up))
    from_near = exchange(sent, NEAR)

    keep, to_core = core_halves(grad_up, gathered, n_c, n_x)
    from_core = send_on(to_core, "c", 1)
    half = add_halves(keep, gathered, from_core, n_x)
    arrived = [half[0]]
    for k in range(1, n_x):
        arrived.append(send_on(half[k], "x", k))
    by_far = sum_and_repack(from_near, n_far, n_zh)
    from_far = exchange(by_far, ("zh", *FAR))

    eighth = sum(block.astype(jnp.float32) for block in arrived).astype(jnp.bfloat16)
    spread = [eighth]
    for k in range(1, n_x):
        spread.append(send_on(eighth, "x", k))
    eighth, x_next = lax.optimization_barrier((eighth, x_next))
    hidden_next = next_branch(x_next, gathered, value_next, conv_taps, conv_bias)
    hidden_next, *spread = lax.optimization_barrier((hidden_next, *spread))
    half = jnp.stack(spread)
    grad_input = put_in_order(half, send_on(half, "c", 1), n_c).reshape(row_count, width)
    from_far, grad_input = lax.optimization_barrier((from_far, grad_input))
    new_w, new_taps, new_bias = last_sum(from_far, sum_w, sum_taps, sum_bias)
    return hidden_next, grad_input, grad_value, new_w, new_taps, new_bias


def solution(mesh):
    n_fs, n_tp = mesh.shape["fs"], mesh.shape["tp"]
    n_y, n_c = 4, 2
    n_z = n_fs // n_y
    fine = Mesh(
        mesh.devices.reshape(mesh.shape["rep"], n_z // 4, 2, 2, n_y, n_tp // n_c, n_c),
        ("zh", *FAR, *NEAR, "x", "c"),
    )
    fs, tp = (*FAR, *NEAR), ("x", "c")
    tokens = ("zh", *fs)
    in_specs = (
        P(tokens, None),
        P(tokens, tp),
        P(tokens, None),
        P(tokens, tp),
        P(tokens, tp),
        P(fs, tp),
        P(None, tp),
        P(tp),
        P(fs, tp),
        P(None, tp),
        P(tp),
    )
    out_specs = (
        P(tokens, tp),
        P(tokens, None),
        P(tokens, tp),
        P(fs, tp),
        P(None, tp),
        P(tp),
    )
    return jax.shard_map(
        per_device, mesh=fine, in_specs=in_specs, out_specs=out_specs, check_vma=False
    )
```

```python
import jax
import jax.numpy as jnp
from jax import lax
from jax.experimental import pallas as pl
from jax.experimental.pallas import tpu as pltpu
from jax.sharding import Mesh
from jax.sharding import PartitionSpec as P


SEQ_LEN = 128
SMALL_ROWS = 8
FAR, NEAR = ("zm", "zp"), ("zl", "y")
FAR_SHIFTS = (0, 1, -1, 2)


def copies_to(block, axis, size):
    copies = jnp.broadcast_to(block, (size, *block.shape))
    return lax.all_to_all(copies, axis, 0, 0, tiled=True)


def exchange(blocks, axis):
    return lax.all_to_all(blocks, axis, 0, 0, tiled=True)


def send_on(block, axis, shift):
    size = lax.axis_size(axis)
    return lax.ppermute(block, axis, [(i, (i + shift + size) % size) for i in range(size)])


def near(array):
    return pltpu.with_memory_space_constraint(array, pltpu.VMEM)


VMEM = pl.BlockSpec(memory_space=pltpu.VMEM)
HBM = pl.BlockSpec(memory_space=pltpu.HBM)


def cost(flops, count, exps=0):
    return pl.CostEstimate(flops=flops, bytes_accessed=count, transcendentals=exps)


def put_in_order(own, other, n_c):
    n_x = own.shape[0]

    def body(own_ref, other_ref, out_ref):
        at_x, at_c = lax.axis_index("x"), lax.axis_index("c")
        for k in range(n_x):
            spot = (at_x + n_x - k) % n_x
            out_ref[at_c * n_x + spot] = own_ref[k]
            out_ref[(1 - at_c) * n_x + spot] = other_ref[k]

    return pl.pallas_call(
        body,
        in_specs=[VMEM] * 2,
        out_shape=jax.ShapeDtypeStruct((n_c * n_x, *own.shape[1:]), own.dtype),
        cost_estimate=cost(0, 8 * own.size),
        name="put_in_order",
        compiler_params=pltpu.CompilerParams(vmem_limit_bytes=24 * 2**20),
    )(near(own), near(other))


EDGE = 8


def later(values, offset):
    if offset == 0:
        return values
    moved = pltpu.roll(values, offset, 0)
    pieces = []
    for start in range(0, values.shape[0], SEQ_LEN):
        edge = moved[start : start + EDGE]
        rows = lax.broadcasted_iota(jnp.int32, edge.shape, 0)
        pieces.append(jnp.where(rows >= offset, edge, 0.0))
        pieces.append(moved[start + EDGE : start + SEQ_LEN])
    return jnp.concatenate(pieces, axis=0)


def earlier(values, offset):
    if offset == 0:
        return values
    moved = pltpu.roll(values, values.shape[0] - offset, 0)
    pieces = []
    for end in range(SEQ_LEN, values.shape[0] + 1, SEQ_LEN):
        pieces.append(moved[end - SEQ_LEN : end - EDGE])
        edge = moved[end - EDGE : end]
        rows = lax.broadcasted_iota(jnp.int32, edge.shape, 0)
        pieces.append(jnp.where(rows < EDGE - offset, edge, 0.0))
    return jnp.concatenate(pieces, axis=0)


def lags_of(up, tap_count):
    return [later(up, tap_count - 1 - j) for j in range(tap_count)]


def gated(lags, taps_ref, bias_ref):
    total = bias_ref[...][None, :]
    for j, lag in enumerate(lags):
        total = total + taps_ref[j : j + 1, :] * lag
    return total


def high_and_low(rows):
    high = rows.astype(jnp.bfloat16).astype(jnp.float32)
    half = SMALL_ROWS // 2
    return (high + pltpu.roll(rows - high, half, 0)).astype(jnp.bfloat16)


def previous_branch(
    x_prev, plane, rest, cotangent, value_prev, conv_taps, conv_bias, grad_scale
):
    row_count, width = x_prev.shape
    n_near, shard_rows, units = plane.shape
    n_far = rest.shape[1] + 1
    tap_count = conv_taps.shape[0]
    each = n_far * shard_rows

    def body(
        x_ref,
        w_ref,
        rest_ref,
        cot_ref,
        value_ref,
        taps_ref,
        bias_ref,
        gv_ref,
        natural_ref,
        gu_ref,
        sent_out,
        sent_ref,
        sems,
    ):
        spots = [
            (near_at, far_at, (far_at * n_near + near_at) * shard_rows)
            for near_at in range(n_near)
            for far_at in range(n_far)
        ]
        own_far = lax.axis_index("zm") * lax.axis_size("zp") + lax.axis_index("zp")
        for near_at in range(n_near):
            for k in range(n_far):
                far_at = (own_far + n_far - FAR_SHIFTS[k]) % n_far
                at = (far_at * n_near + near_at) * shard_rows
                block = w_ref[near_at] if k == 0 else rest_ref[near_at, k - 1]
                natural_ref[pl.ds(pl.multiple_of(at, shard_rows), shard_rows)] = block
        up = jnp.dot(x_ref[...], natural_ref[...], preferred_element_type=jnp.float32)
        up = up.astype(jnp.bfloat16).astype(jnp.float32)
        lags = lags_of(up, tap_count)
        gate = gated(lags, taps_ref, bias_ref)
        sig = jax.nn.sigmoid(gate)
        cot = cot_ref[...].astype(jnp.float32)
        gv_ref[...] = (cot * gate * sig).astype(jnp.bfloat16)
        grad_gate = cot * value_ref[...].astype(jnp.float32) * sig * (1.0 + gate * (1.0 - sig))
        grad_up = jnp.zeros_like(grad_gate)
        for j in range(tap_count):
            grad_up = grad_up + taps_ref[j : j + 1, :] * earlier(grad_gate, tap_count - 1 - j)
        gu_ref[...] = grad_up.astype(jnp.bfloat16)

        grad_w = lax.dot_general(
            x_ref[...], gu_ref[...], (((0,), (0,)), ((), ())), preferred_element_type=jnp.float32
        )
        grad_w = (grad_w * grad_scale).astype(jnp.bfloat16)
        sums = [
            jnp.sum(grad_gate * lag, axis=0, keepdims=True) for lag in lags
        ] + [jnp.sum(grad_gate, axis=0, keepdims=True)]
        rest = jnp.zeros((SMALL_ROWS - len(sums), units), jnp.float32)
        small = high_and_low(jnp.concatenate([*sums, rest], axis=0) * grad_scale)
        moves = []
        for block in range(n_near):
            for near_at, far_at, at in spots:
                if near_at == block:
                    to = far_at * shard_rows
                    sent_ref[block, to : to + shard_rows] = grad_w[at : at + shard_rows]
            sent_ref[block, each:] = small
            moves.append(
                pltpu.make_async_copy(sent_ref.at[block], sent_out.at[block], sems.at[block])
            )
            moves[-1].start()
        for move in moves:
            move.wait()

    half = jnp.bfloat16
    return pl.pallas_call(
        body,
        in_specs=[VMEM] * 7,
        out_specs=[pl.BlockSpec(), VMEM, VMEM, HBM],
        out_shape=[
            jax.ShapeDtypeStruct((row_count, units), half),
            pltpu.VMEM((width, units), half),
            pltpu.VMEM((row_count, units), half),
            pltpu.HBM((n_near, each + SMALL_ROWS, units), half),
        ],
        scratch_shapes=[
            pltpu.VMEM((n_near, each + SMALL_ROWS, units), half),
            pltpu.SemaphoreType.DMA((n_near,)),
        ],
        cost_estimate=cost(4 * row_count * width * units, 8 * width * units, row_count * units),
        name="previous_branch",
        compiler_params=pltpu.CompilerParams(vmem_limit_bytes=24 * 2**20),
    )(
        near(x_prev),
        near(plane),
        near(rest),
        near(cotangent),
        near(value_prev),
        near(conv_taps),
        near(conv_bias),
    )


def core_halves(grad_up, weights, n_c, n_x):
    row_count, units = grad_up.shape
    width = weights.shape[0]
    half_rows = row_count // n_c
    block_rows = half_rows // n_x

    def body(gu_ref, natural_ref, keep_ref, send_out, turned_ref, send_ref, sem):
        at_x, at_c = lax.axis_index("x"), lax.axis_index("c")
        for i, half_ref in ((1, turned_ref), (0, keep_ref)):
            core = (at_c + i) % n_c
            for k in range(n_x):
                row = core * half_rows + ((at_x + k) % n_x) * block_rows
                half_ref[k * block_rows : (k + 1) * block_rows] = gu_ref[
                    pl.ds(pl.multiple_of(row, block_rows), block_rows)
                ]
        send_ref[...] = lax.dot_general(
            turned_ref[...],
            natural_ref[...],
            (((1,), (1,)), ((), ())),
            preferred_element_type=jnp.float32,
        ).astype(jnp.bfloat16)
        move = pltpu.make_async_copy(send_ref, send_out, sem)
        move.start()
        move.wait()

    half = jnp.bfloat16
    return pl.pallas_call(
        body,
        in_specs=[VMEM] * 2,
        out_specs=[VMEM, HBM],
        out_shape=[pltpu.VMEM((half_rows, units), half), pltpu.HBM((half_rows, width), half)],
        scratch_shapes=[
            pltpu.VMEM((half_rows, units), half),
            pltpu.VMEM((half_rows, width), half),
            pltpu.SemaphoreType.DMA(()),
        ],
        cost_estimate=cost(row_count * width * units, 4 * width * units),
        name="core_halves",
        compiler_params=pltpu.CompilerParams(vmem_limit_bytes=16 * 2**20),
    )(near(grad_up), near(weights))


def add_halves(keep, weights, from_core, n_x):
    rows, width = from_core.shape
    each = rows // n_x

    def body(keep_ref, w_ref, other_ref, *refs):
        out_refs, blocks_ref, sems = refs[:n_x], refs[n_x], refs[n_x + 1]
        total = lax.dot_general(
            keep_ref[...],
            w_ref[...],
            (((1,), (1,)), ((), ())),
            preferred_element_type=jnp.float32,
        )
        total = (total + other_ref[...].astype(jnp.float32)).astype(jnp.bfloat16)
        moves = []
        for k in range(n_x):
            blocks_ref[k] = total[k * each : (k + 1) * each]
            moves.append(pltpu.make_async_copy(blocks_ref.at[k], out_refs[k], sems.at[k]))
            moves[-1].start()
        for move in moves:
            move.wait()

    return pl.pallas_call(
        body,
        in_specs=[VMEM] * 3,
        out_specs=[HBM] * n_x,
        out_shape=[pltpu.HBM((each, width), jnp.bfloat16)] * n_x,
        scratch_shapes=[
            pltpu.VMEM((n_x, each, width), jnp.bfloat16),
            pltpu.SemaphoreType.DMA((n_x,)),
        ],
        cost_estimate=cost(2 * keep.size * width, 8 * weights.size),
        name="add_halves",
        compiler_params=pltpu.CompilerParams(vmem_limit_bytes=16 * 2**20),
    )(near(keep), near(weights), near(from_core))


def next_branch(x_next, weights, value_next, conv_taps, conv_bias):
    row_count, width = x_next.shape
    units = weights.shape[1]

    def body(x_ref, w_ref, value_ref, taps_ref, bias_ref, out_ref):
        up = jnp.dot(x_ref[...], w_ref[...], preferred_element_type=jnp.float32)
        up = up.astype(jnp.bfloat16).astype(jnp.float32)
        gate = gated(lags_of(up, taps_ref.shape[0]), taps_ref, bias_ref)
        hidden = gate * jax.nn.sigmoid(gate) * value_ref[...].astype(jnp.float32)
        out_ref[...] = hidden.astype(jnp.bfloat16)

    return pl.pallas_call(
        body,
        in_specs=[VMEM] * 5,
        out_shape=jax.ShapeDtypeStruct((row_count, units), jnp.bfloat16),
        cost_estimate=cost(2 * row_count * width * units, 4 * width * units, row_count * units),
        name="next_branch",
        compiler_params=pltpu.CompilerParams(vmem_limit_bytes=24 * 2**20),
    )(near(x_next), near(weights), near(value_next), near(conv_taps), near(conv_bias))


def summed(block):
    return jnp.sum(block.astype(jnp.float32), axis=0)


def small_total(block):
    total = summed(block)
    half = SMALL_ROWS // 2
    rows = lax.broadcasted_iota(jnp.int32, total.shape, 0)
    return jnp.where(rows < half, total + pltpu.roll(total, half, 0), 0.0)


def sum_and_repack(arrived, parts, repeats):
    _, rows, units = arrived.shape
    extra = SMALL_ROWS
    each = (rows - extra) // parts

    def body(in_ref, out_ref, block_ref, sems):
        small = high_and_low(small_total(in_ref[:, rows - extra :]))
        moves = []
        for p in range(parts):
            main = summed(in_ref[:, p * each : (p + 1) * each]).astype(jnp.bfloat16)
            block_ref[p, :each] = main
            block_ref[p, each:] = small
            for r in range(repeats):
                to = r * parts + p
                move = pltpu.make_async_copy(block_ref.at[p], out_ref.at[to], sems.at[to])
                move.start()
                moves.append(move)
        for move in moves:
            move.wait()

    return pl.pallas_call(
        body,
        in_specs=[VMEM],
        out_specs=HBM,
        out_shape=pltpu.HBM((repeats * parts, each + extra, units), jnp.bfloat16),
        scratch_shapes=[
            pltpu.VMEM((parts, each + extra, units), jnp.bfloat16),
            pltpu.SemaphoreType.DMA((repeats * parts,)),
        ],
        cost_estimate=cost(2 * arrived.size, 4 * arrived.size),
        name="sum_and_repack",
        compiler_params=pltpu.CompilerParams(vmem_limit_bytes=24 * 2**20),
    )(near(arrived))


def last_sum(arrived, sum_w, sum_taps, sum_bias):
    rows, _ = sum_w.shape
    tap_count = sum_taps.shape[0]

    def body(in_ref, w_ref, taps_ref, bias_ref, new_w_ref, new_taps_ref, new_bias_ref):
        new_w_ref[...] = w_ref[...] + summed(in_ref[:, :rows])
        small = small_total(in_ref[:, rows:])
        new_taps_ref[...] = taps_ref[...] + small[:tap_count]
        new_bias_ref[...] = bias_ref[...] + small[tap_count]

    return pl.pallas_call(
        body,
        in_specs=[VMEM] * 4,
        out_shape=[
            jax.ShapeDtypeStruct(sum_w.shape, jnp.float32),
            jax.ShapeDtypeStruct(sum_taps.shape, jnp.float32),
            jax.ShapeDtypeStruct(sum_bias.shape, jnp.float32),
        ],
        cost_estimate=cost(2 * arrived.size, 4 * arrived.size),
        name="last_sum",
        compiler_params=pltpu.CompilerParams(vmem_limit_bytes=24 * 2**20),
    )(near(arrived), near(sum_w), near(sum_taps), near(sum_bias))


def per_device(
    x_next,
    value_next,
    x_prev,
    value_prev,
    cotangent,
    w_gate,
    conv_taps,
    conv_bias,
    sum_w,
    sum_taps,
    sum_bias,
):
    row_count, width = x_next.shape
    n_zh, n_x, n_c = (lax.axis_size(a) for a in ("zh", "x", "c"))
    n_far, n_near = lax.axis_size(FAR), lax.axis_size(NEAR)

    plane = copies_to(w_gate, NEAR, n_near)
    far_shards = [send_on(w_gate, ("zh", *FAR), shift) for shift in FAR_SHIFTS[1:]]
    rest = copies_to(jnp.stack(far_shards), NEAR, n_near)
    grad_scale = float(row_count * n_zh * n_far * n_near) ** (-0.5)
    grad_value, gathered, grad_up, sent = previous_branch(
        x_prev, plane, rest, cotangent, value_prev, conv_taps, conv_bias, grad_scale
    )
    sent, grad_up = lax.optimization_barrier((sent, grad_up))
    from_near = exchange(sent, NEAR)

    keep, to_core = core_halves(grad_up, gathered, n_c, n_x)
    from_core = send_on(to_core, "c", 1)
    half = add_halves(keep, gathered, from_core, n_x)
    arrived = [half[0]]
    for k in range(1, n_x):
        arrived.append(send_on(half[k], "x", k))
    by_far = sum_and_repack(from_near, n_far, n_zh)
    from_far = exchange(by_far, ("zh", *FAR))

    eighth = sum(block.astype(jnp.float32) for block in arrived).astype(jnp.bfloat16)
    spread = [eighth]
    for k in range(1, n_x):
        spread.append(send_on(eighth, "x", k))
    eighth, x_next = lax.optimization_barrier((eighth, x_next))
    hidden_next = next_branch(x_next, gathered, value_next, conv_taps, conv_bias)
    hidden_next, *spread = lax.optimization_barrier((hidden_next, *spread))
    half = jnp.stack(spread)
    grad_input = put_in_order(half, send_on(half, "c", 1), n_c).reshape(row_count, width)
    from_far, grad_input = lax.optimization_barrier((from_far, grad_input))
    new_w, new_taps, new_bias = last_sum(from_far, sum_w, sum_taps, sum_bias)
    return hidden_next, grad_input, grad_value, new_w, new_taps, new_bias


def solution(mesh):
    n_fs, n_tp = mesh.shape["fs"], mesh.shape["tp"]
    n_y, n_c = 4, 2
    n_z = n_fs // n_y
    fine = Mesh(
        mesh.devices.reshape(mesh.shape["rep"], n_z // 4, 2, 2, n_y, n_tp // n_c, n_c),
        ("zh", *FAR, *NEAR, "x", "c"),
    )
    fs, tp = (*FAR, *NEAR), ("x", "c")
    tokens = ("zh", *fs)
    in_specs = (
        P(tokens, None),
        P(tokens, tp),
        P(tokens, None),
        P(tokens, tp),
        P(tokens, tp),
        P(fs, tp),
        P(None, tp),
        P(tp),
        P(fs, tp),
        P(None, tp),
        P(tp),
    )
    out_specs = (
        P(tokens, tp),
        P(tokens, None),
        P(tokens, tp),
        P(fs, tp),
        P(None, tp),
        P(tp),
    )
    return jax.shard_map(
        per_device, mesh=fine, in_specs=in_specs, out_specs=out_specs, check_vma=False
    )
```

```python
import jax
import jax.numpy as jnp
from jax import lax
from jax.experimental import pallas as pl
from jax.experimental.pallas import tpu as pltpu
from jax.sharding import Mesh
from jax.sharding import PartitionSpec as P


SEQ_LEN = 128
SMALL_ROWS = 8
FAR, NEAR = ("zm", "zp"), ("zl", "y")
FAR_SHIFTS = (0, 1, -1, 2)


def copies_to(block, axis, size):
    copies = jnp.broadcast_to(block, (size, *block.shape))
    return lax.all_to_all(copies, axis, 0, 0, tiled=True)


def exchange(blocks, axis):
    return lax.all_to_all(blocks, axis, 0, 0, tiled=True)


def send_on(block, axis, shift):
    size = lax.axis_size(axis)
    return lax.ppermute(block, axis, [(i, (i + shift + size) % size) for i in range(size)])


def near(array):
    return pltpu.with_memory_space_constraint(array, pltpu.VMEM)


VMEM = pl.BlockSpec(memory_space=pltpu.VMEM)
HBM = pl.BlockSpec(memory_space=pltpu.HBM)


def cost(flops, count, exps=0):
    return pl.CostEstimate(flops=flops, bytes_accessed=count, transcendentals=exps)


def put_in_order(own, other, n_c):
    n_x = own.shape[0]

    def body(own_ref, other_ref, out_ref):
        at_x, at_c = lax.axis_index("x"), lax.axis_index("c")
        for k in range(n_x):
            spot = (at_x + n_x - k) % n_x
            out_ref[at_c * n_x + spot] = own_ref[k]
            out_ref[(1 - at_c) * n_x + spot] = other_ref[k]

    return pl.pallas_call(
        body,
        in_specs=[VMEM] * 2,
        out_shape=jax.ShapeDtypeStruct((n_c * n_x, *own.shape[1:]), own.dtype),
        cost_estimate=cost(0, 8 * own.size),
        name="put_in_order",
        compiler_params=pltpu.CompilerParams(vmem_limit_bytes=24 * 2**20),
    )(near(own), near(other))


EDGE = 8


def later(values, offset):
    if offset == 0:
        return values
    moved = pltpu.roll(values, offset, 0)
    pieces = []
    for start in range(0, values.shape[0], SEQ_LEN):
        edge = moved[start : start + EDGE]
        rows = lax.broadcasted_iota(jnp.int32, edge.shape, 0)
        pieces.append(jnp.where(rows >= offset, edge, 0.0))
        pieces.append(moved[start + EDGE : start + SEQ_LEN])
    return jnp.concatenate(pieces, axis=0)


def earlier(values, offset):
    if offset == 0:
        return values
    moved = pltpu.roll(values, values.shape[0] - offset, 0)
    pieces = []
    for end in range(SEQ_LEN, values.shape[0] + 1, SEQ_LEN):
        pieces.append(moved[end - SEQ_LEN : end - EDGE])
        edge = moved[end - EDGE : end]
        rows = lax.broadcasted_iota(jnp.int32, edge.shape, 0)
        pieces.append(jnp.where(rows < EDGE - offset, edge, 0.0))
    return jnp.concatenate(pieces, axis=0)


def lags_of(up, tap_count):
    return [later(up, tap_count - 1 - j) for j in range(tap_count)]


def gated(lags, taps_ref, bias_ref):
    total = bias_ref[...][None, :]
    for j, lag in enumerate(lags):
        total = total + taps_ref[j : j + 1, :] * lag
    return total


def high_and_low(rows):
    high = rows.astype(jnp.bfloat16).astype(jnp.float32)
    half = SMALL_ROWS // 2
    return (high + pltpu.roll(rows - high, half, 0)).astype(jnp.bfloat16)


def previous_branch(
    x_prev, plane, rest, cotangent, value_prev, conv_taps, conv_bias, grad_scale, n_c
):
    row_count, width = x_prev.shape
    n_near, shard_rows, units = plane.shape
    n_far = rest.shape[1] + 1
    tap_count = conv_taps.shape[0]
    n_x = lax.axis_size("x")
    half_rows = row_count // n_c
    block_rows = half_rows // n_x
    each = n_far * shard_rows

    def body(
        x_ref,
        w_ref,
        rest_ref,
        cot_ref,
        value_ref,
        taps_ref,
        bias_ref,
        gv_ref,
        natural_ref,
        keep_ref,
        send_out,
        sent_out,
        gu_ref,
        turned_ref,
        send_ref,
        sent_ref,
        sems,
    ):
        spots = [
            (near_at, far_at, (far_at * n_near + near_at) * shard_rows)
            for near_at in range(n_near)
            for far_at in range(n_far)
        ]
        own_far = lax.axis_index("zm") * lax.axis_size("zp") + lax.axis_index("zp")
        for near_at in range(n_near):
            for k in range(n_far):
                far_at = (own_far + n_far - FAR_SHIFTS[k]) % n_far
                at = (far_at * n_near + near_at) * shard_rows
                block = w_ref[near_at] if k == 0 else rest_ref[near_at, k - 1]
                natural_ref[pl.ds(pl.multiple_of(at, shard_rows), shard_rows)] = block
        up = jnp.dot(x_ref[...], natural_ref[...], preferred_element_type=jnp.float32)
        up = up.astype(jnp.bfloat16).astype(jnp.float32)
        lags = lags_of(up, tap_count)
        gate = gated(lags, taps_ref, bias_ref)
        sig = jax.nn.sigmoid(gate)
        cot = cot_ref[...].astype(jnp.float32)
        gv_ref[...] = (cot * gate * sig).astype(jnp.bfloat16)
        grad_gate = cot * value_ref[...].astype(jnp.float32) * sig * (1.0 + gate * (1.0 - sig))
        grad_up = jnp.zeros_like(grad_gate)
        for j in range(tap_count):
            grad_up = grad_up + taps_ref[j : j + 1, :] * earlier(grad_gate, tap_count - 1 - j)
        gu_ref[...] = grad_up.astype(jnp.bfloat16)

        at_x, at_c = lax.axis_index("x"), lax.axis_index("c")
        for i, half_ref in ((1, turned_ref), (0, keep_ref)):
            core = (at_c + i) % n_c
            for k in range(n_x):
                row = core * half_rows + ((at_x + k) % n_x) * block_rows
                half_ref[k * block_rows : (k + 1) * block_rows] = gu_ref[
                    pl.ds(pl.multiple_of(row, block_rows), block_rows)
                ]
        send_ref[...] = lax.dot_general(
            turned_ref[...],
            natural_ref[...],
            (((1,), (1,)), ((), ())),
            preferred_element_type=jnp.float32,
        ).astype(jnp.bfloat16)
        moves = [pltpu.make_async_copy(send_ref, send_out, sems.at[n_near])]
        moves[0].start()

        grad_w = lax.dot_general(
            x_ref[...], gu_ref[...], (((0,), (0,)), ((), ())), preferred_element_type=jnp.float32
        )
        grad_w = (grad_w * grad_scale).astype(jnp.bfloat16)
        sums = [
            jnp.sum(grad_gate * lag, axis=0, keepdims=True) for lag in lags
        ] + [jnp.sum(grad_gate, axis=0, keepdims=True)]
        rest = jnp.zeros((SMALL_ROWS - len(sums), units), jnp.float32)
        small = high_and_low(jnp.concatenate([*sums, rest], axis=0) * grad_scale)
        for block in range(n_near):
            for near_at, far_at, at in spots:
                if near_at == block:
                    to = far_at * shard_rows
                    sent_ref[block, to : to + shard_rows] = grad_w[at : at + shard_rows]
            sent_ref[block, each:] = small
            moves.append(
                pltpu.make_async_copy(sent_ref.at[block], sent_out.at[block], sems.at[block])
            )
            moves[-1].start()
        for move in moves:
            move.wait()

    half = jnp.bfloat16
    return pl.pallas_call(
        body,
        in_specs=[VMEM] * 7,
        out_specs=[pl.BlockSpec(), VMEM, VMEM, HBM, HBM],
        out_shape=[
            jax.ShapeDtypeStruct((row_count, units), half),
            pltpu.VMEM((width, units), half),
            pltpu.VMEM((half_rows, units), half),
            pltpu.HBM((half_rows, width), half),
            pltpu.HBM((n_near, each + SMALL_ROWS, units), half),
        ],
        scratch_shapes=[
            pltpu.VMEM((row_count, units), half),
            pltpu.VMEM((half_rows, units), half),
            pltpu.VMEM((half_rows, width), half),
            pltpu.VMEM((n_near, each + SMALL_ROWS, units), half),
            pltpu.SemaphoreType.DMA((n_near + 1,)),
        ],
        cost_estimate=cost(5 * row_count * width * units, 8 * width * units, row_count * units),
        name="previous_branch",
        compiler_params=pltpu.CompilerParams(vmem_limit_bytes=24 * 2**20),
    )(
        near(x_prev),
        near(plane),
        near(rest),
        near(cotangent),
        near(value_prev),
        near(conv_taps),
        near(conv_bias),
    )


def add_halves(keep, weights, from_core, n_x):
    rows, width = from_core.shape
    each = rows // n_x

    def body(keep_ref, w_ref, other_ref, *refs):
        out_refs, blocks_ref, sems = refs[:n_x], refs[n_x], refs[n_x + 1]
        total = lax.dot_general(
            keep_ref[...],
            w_ref[...],
            (((1,), (1,)), ((), ())),
            preferred_element_type=jnp.float32,
        )
        total = (total + other_ref[...].astype(jnp.float32)).astype(jnp.bfloat16)
        moves = []
        for k in range(n_x):
            blocks_ref[k] = total[k * each : (k + 1) * each]
            moves.append(pltpu.make_async_copy(blocks_ref.at[k], out_refs[k], sems.at[k]))
            moves[-1].start()
        for move in moves:
            move.wait()

    return pl.pallas_call(
        body,
        in_specs=[VMEM] * 3,
        out_specs=[HBM] * n_x,
        out_shape=[pltpu.HBM((each, width), jnp.bfloat16)] * n_x,
        scratch_shapes=[
            pltpu.VMEM((n_x, each, width), jnp.bfloat16),
            pltpu.SemaphoreType.DMA((n_x,)),
        ],
        cost_estimate=cost(2 * keep.size * width, 8 * weights.size),
        name="add_halves",
        compiler_params=pltpu.CompilerParams(vmem_limit_bytes=16 * 2**20),
    )(near(keep), near(weights), near(from_core))


def next_branch(x_next, weights, value_next, conv_taps, conv_bias):
    row_count, width = x_next.shape
    units = weights.shape[1]

    def body(x_ref, w_ref, value_ref, taps_ref, bias_ref, out_ref):
        up = jnp.dot(x_ref[...], w_ref[...], preferred_element_type=jnp.float32)
        up = up.astype(jnp.bfloat16).astype(jnp.float32)
        gate = gated(lags_of(up, taps_ref.shape[0]), taps_ref, bias_ref)
        hidden = gate * jax.nn.sigmoid(gate) * value_ref[...].astype(jnp.float32)
        out_ref[...] = hidden.astype(jnp.bfloat16)

    return pl.pallas_call(
        body,
        in_specs=[VMEM] * 5,
        out_shape=jax.ShapeDtypeStruct((row_count, units), jnp.bfloat16),
        cost_estimate=cost(2 * row_count * width * units, 4 * width * units, row_count * units),
        name="next_branch",
        compiler_params=pltpu.CompilerParams(vmem_limit_bytes=24 * 2**20),
    )(near(x_next), near(weights), near(value_next), near(conv_taps), near(conv_bias))


def summed(block):
    return jnp.sum(block.astype(jnp.float32), axis=0)


def small_total(block):
    total = summed(block)
    half = SMALL_ROWS // 2
    rows = lax.broadcasted_iota(jnp.int32, total.shape, 0)
    return jnp.where(rows < half, total + pltpu.roll(total, half, 0), 0.0)


def sum_and_repack(arrived, parts, repeats):
    _, rows, units = arrived.shape
    extra = SMALL_ROWS
    each = (rows - extra) // parts

    def body(in_ref, out_ref, block_ref, sems):
        small = high_and_low(small_total(in_ref[:, rows - extra :]))
        moves = []
        for p in range(parts):
            main = summed(in_ref[:, p * each : (p + 1) * each]).astype(jnp.bfloat16)
            block_ref[p, :each] = main
            block_ref[p, each:] = small
            for r in range(repeats):
                to = r * parts + p
                move = pltpu.make_async_copy(block_ref.at[p], out_ref.at[to], sems.at[to])
                move.start()
                moves.append(move)
        for move in moves:
            move.wait()

    return pl.pallas_call(
        body,
        in_specs=[VMEM],
        out_specs=HBM,
        out_shape=pltpu.HBM((repeats * parts, each + extra, units), jnp.bfloat16),
        scratch_shapes=[
            pltpu.VMEM((parts, each + extra, units), jnp.bfloat16),
            pltpu.SemaphoreType.DMA((repeats * parts,)),
        ],
        cost_estimate=cost(2 * arrived.size, 4 * arrived.size),
        name="sum_and_repack",
        compiler_params=pltpu.CompilerParams(vmem_limit_bytes=24 * 2**20),
    )(near(arrived))


def last_sum(arrived, sum_w, sum_taps, sum_bias):
    rows, _ = sum_w.shape
    tap_count = sum_taps.shape[0]

    def body(in_ref, w_ref, taps_ref, bias_ref, new_w_ref, new_taps_ref, new_bias_ref):
        new_w_ref[...] = w_ref[...] + summed(in_ref[:, :rows])
        small = small_total(in_ref[:, rows:])
        new_taps_ref[...] = taps_ref[...] + small[:tap_count]
        new_bias_ref[...] = bias_ref[...] + small[tap_count]

    return pl.pallas_call(
        body,
        in_specs=[VMEM] * 4,
        out_shape=[
            jax.ShapeDtypeStruct(sum_w.shape, jnp.float32),
            jax.ShapeDtypeStruct(sum_taps.shape, jnp.float32),
            jax.ShapeDtypeStruct(sum_bias.shape, jnp.float32),
        ],
        cost_estimate=cost(2 * arrived.size, 4 * arrived.size),
        name="last_sum",
        compiler_params=pltpu.CompilerParams(vmem_limit_bytes=24 * 2**20),
    )(near(arrived), near(sum_w), near(sum_taps), near(sum_bias))


def per_device(
    x_next,
    value_next,
    x_prev,
    value_prev,
    cotangent,
    w_gate,
    conv_taps,
    conv_bias,
    sum_w,
    sum_taps,
    sum_bias,
):
    row_count, width = x_next.shape
    n_zh, n_x, n_c = (lax.axis_size(a) for a in ("zh", "x", "c"))
    n_far, n_near = lax.axis_size(FAR), lax.axis_size(NEAR)

    plane = copies_to(w_gate, NEAR, n_near)
    far_shards = [send_on(w_gate, ("zh", *FAR), shift) for shift in FAR_SHIFTS[1:]]
    rest = copies_to(jnp.stack(far_shards), NEAR, n_near)
    grad_scale = float(row_count * n_zh * n_far * n_near) ** (-0.5)
    grad_value, gathered, keep, to_core, sent = previous_branch(
        x_prev, plane, rest, cotangent, value_prev, conv_taps, conv_bias, grad_scale, n_c
    )
    from_core = send_on(to_core, "c", 1)
    from_near = exchange(sent, NEAR)

    half = add_halves(keep, gathered, from_core, n_x)
    arrived = [half[0]]
    for k in range(1, n_x):
        arrived.append(send_on(half[k], "x", k))
    by_far = sum_and_repack(from_near, n_far, n_zh)
    from_far = exchange(by_far, ("zh", *FAR))

    eighth = sum(block.astype(jnp.float32) for block in arrived).astype(jnp.bfloat16)
    spread = [eighth]
    for k in range(1, n_x):
        spread.append(send_on(eighth, "x", k))
    eighth, x_next = lax.optimization_barrier((eighth, x_next))
    hidden_next = next_branch(x_next, gathered, value_next, conv_taps, conv_bias)
    hidden_next, *spread = lax.optimization_barrier((hidden_next, *spread))
    half = jnp.stack(spread)
    grad_input = put_in_order(half, send_on(half, "c", 1), n_c).reshape(row_count, width)
    from_far, grad_input = lax.optimization_barrier((from_far, grad_input))
    new_w, new_taps, new_bias = last_sum(from_far, sum_w, sum_taps, sum_bias)
    return hidden_next, grad_input, grad_value, new_w, new_taps, new_bias


def solution(mesh):
    n_fs, n_tp = mesh.shape["fs"], mesh.shape["tp"]
    n_y, n_c = 4, 2
    n_z = n_fs // n_y
    fine = Mesh(
        mesh.devices.reshape(mesh.shape["rep"], n_z // 4, 2, 2, n_y, n_tp // n_c, n_c),
        ("zh", *FAR, *NEAR, "x", "c"),
    )
    fs, tp = (*FAR, *NEAR), ("x", "c")
    tokens = ("zh", *fs)
    in_specs = (
        P(tokens, None),
        P(tokens, tp),
        P(tokens, None),
        P(tokens, tp),
        P(tokens, tp),
        P(fs, tp),
        P(None, tp),
        P(tp),
        P(fs, tp),
        P(None, tp),
        P(tp),
    )
    out_specs = (
        P(tokens, tp),
        P(tokens, None),
        P(tokens, tp),
        P(fs, tp),
        P(None, tp),
        P(tp),
    )
    return jax.shard_map(
        per_device, mesh=fine, in_specs=in_specs, out_specs=out_specs, check_vma=False
    )
```

```python
import jax
import jax.numpy as jnp
from jax import lax
from jax.experimental import pallas as pl
from jax.experimental.pallas import tpu as pltpu
from jax.sharding import Mesh
from jax.sharding import PartitionSpec as P


SEQ_LEN = 128
SMALL_ROWS = 8
FAR, NEAR = ("zm", "zp"), ("zl", "y")


def copies_to(block, axis, size):
    copies = jnp.broadcast_to(block, (size, *block.shape))
    return lax.all_to_all(copies, axis, 0, 0, tiled=True)


def exchange(blocks, axis):
    return lax.all_to_all(blocks, axis, 0, 0, tiled=True)


def send_on(block, axis, shift):
    size = lax.axis_size(axis)
    return lax.ppermute(block, axis, [(i, (i + shift) % size) for i in range(size)])


def near(array):
    return pltpu.with_memory_space_constraint(array, pltpu.VMEM)


VMEM = pl.BlockSpec(memory_space=pltpu.VMEM)
HBM = pl.BlockSpec(memory_space=pltpu.HBM)


def cost(flops, count, exps=0):
    return pl.CostEstimate(flops=flops, bytes_accessed=count, transcendentals=exps)


def put_in_order(own, other, n_c):
    n_x = own.shape[0]

    def body(own_ref, other_ref, out_ref):
        at_x, at_c = lax.axis_index("x"), lax.axis_index("c")
        for k in range(n_x):
            spot = (at_x + n_x - k) % n_x
            out_ref[at_c * n_x + spot] = own_ref[k]
            out_ref[(1 - at_c) * n_x + spot] = other_ref[k]

    return pl.pallas_call(
        body,
        in_specs=[VMEM] * 2,
        out_shape=jax.ShapeDtypeStruct((n_c * n_x, *own.shape[1:]), own.dtype),
        cost_estimate=cost(0, 8 * own.size),
        name="put_in_order",
        compiler_params=pltpu.CompilerParams(vmem_limit_bytes=24 * 2**20),
    )(near(own), near(other))


EDGE = 8


def later(values, offset):
    if offset == 0:
        return values
    moved = pltpu.roll(values, offset, 0)
    pieces = []
    for start in range(0, values.shape[0], SEQ_LEN):
        edge = moved[start : start + EDGE]
        rows = lax.broadcasted_iota(jnp.int32, edge.shape, 0)
        pieces.append(jnp.where(rows >= offset, edge, 0.0))
        pieces.append(moved[start + EDGE : start + SEQ_LEN])
    return jnp.concatenate(pieces, axis=0)


def earlier(values, offset):
    if offset == 0:
        return values
    moved = pltpu.roll(values, values.shape[0] - offset, 0)
    pieces = []
    for end in range(SEQ_LEN, values.shape[0] + 1, SEQ_LEN):
        pieces.append(moved[end - SEQ_LEN : end - EDGE])
        edge = moved[end - EDGE : end]
        rows = lax.broadcasted_iota(jnp.int32, edge.shape, 0)
        pieces.append(jnp.where(rows < EDGE - offset, edge, 0.0))
    return jnp.concatenate(pieces, axis=0)


def lags_of(up, tap_count):
    return [later(up, tap_count - 1 - j) for j in range(tap_count)]


def gated(lags, taps_ref, bias_ref):
    total = bias_ref[...][None, :]
    for j, lag in enumerate(lags):
        total = total + taps_ref[j : j + 1, :] * lag
    return total


def high_and_low(rows):
    high = rows.astype(jnp.bfloat16).astype(jnp.float32)
    half = SMALL_ROWS // 2
    return (high + pltpu.roll(rows - high, half, 0)).astype(jnp.bfloat16)


def previous_branch(x_prev, plane, cotangent, value_prev, conv_taps, conv_bias, grad_scale, n_c):
    row_count, width = x_prev.shape
    n_near, n_far, shard_rows, units = plane.shape
    tap_count = conv_taps.shape[0]
    n_x = lax.axis_size("x")
    half_rows = row_count // n_c
    block_rows = half_rows // n_x
    each = n_far * shard_rows

    def body(
        x_ref,
        w_ref,
        cot_ref,
        value_ref,
        taps_ref,
        bias_ref,
        gv_ref,
        natural_ref,
        keep_ref,
        send_out,
        sent_out,
        gu_ref,
        turned_ref,
        send_ref,
        sent_ref,
        sems,
    ):
        spots = [
            (near_at, far_at, (far_at * n_near + near_at) * shard_rows)
            for near_at in range(n_near)
            for far_at in range(n_far)
        ]
        for near_at, far_at, at in spots:
            natural_ref[at : at + shard_rows] = w_ref[near_at, far_at]
        up = jnp.dot(x_ref[...], natural_ref[...], preferred_element_type=jnp.float32)
        up = up.astype(jnp.bfloat16).astype(jnp.float32)
        lags = lags_of(up, tap_count)
        gate = gated(lags, taps_ref, bias_ref)
        sig = jax.nn.sigmoid(gate)
        cot = cot_ref[...].astype(jnp.float32)
        gv_ref[...] = (cot * gate * sig).astype(jnp.bfloat16)
        grad_gate = cot * value_ref[...].astype(jnp.float32) * sig * (1.0 + gate * (1.0 - sig))
        grad_up = jnp.zeros_like(grad_gate)
        for j in range(tap_count):
            grad_up = grad_up + taps_ref[j : j + 1, :] * earlier(grad_gate, tap_count - 1 - j)
        gu_ref[...] = grad_up.astype(jnp.bfloat16)

        at_x, at_c = lax.axis_index("x"), lax.axis_index("c")
        for i, half_ref in ((1, turned_ref), (0, keep_ref)):
            core = (at_c + i) % n_c
            for k in range(n_x):
                row = core * half_rows + ((at_x + k) % n_x) * block_rows
                half_ref[k * block_rows : (k + 1) * block_rows] = gu_ref[
                    pl.ds(pl.multiple_of(row, block_rows), block_rows)
                ]
        send_ref[...] = lax.dot_general(
            turned_ref[...],
            natural_ref[...],
            (((1,), (1,)), ((), ())),
            preferred_element_type=jnp.float32,
        ).astype(jnp.bfloat16)
        moves = [pltpu.make_async_copy(send_ref, send_out, sems.at[n_near])]
        moves[0].start()

        grad_w = lax.dot_general(
            x_ref[...], gu_ref[...], (((0,), (0,)), ((), ())), preferred_element_type=jnp.float32
        )
        grad_w = (grad_w * grad_scale).astype(jnp.bfloat16)
        sums = [
            jnp.sum(grad_gate * lag, axis=0, keepdims=True) for lag in lags
        ] + [jnp.sum(grad_gate, axis=0, keepdims=True)]
        rest = jnp.zeros((SMALL_ROWS - len(sums), units), jnp.float32)
        small = high_and_low(jnp.concatenate([*sums, rest], axis=0) * grad_scale)
        for block in range(n_near):
            for near_at, far_at, at in spots:
                if near_at == block:
                    to = far_at * shard_rows
                    sent_ref[block, to : to + shard_rows] = grad_w[at : at + shard_rows]
            sent_ref[block, each:] = small
            moves.append(
                pltpu.make_async_copy(sent_ref.at[block], sent_out.at[block], sems.at[block])
            )
            moves[-1].start()
        for move in moves:
            move.wait()

    half = jnp.bfloat16
    return pl.pallas_call(
        body,
        in_specs=[VMEM] * 6,
        out_specs=[pl.BlockSpec(), VMEM, VMEM, HBM, HBM],
        out_shape=[
            jax.ShapeDtypeStruct((row_count, units), half),
            pltpu.VMEM((width, units), half),
            pltpu.VMEM((half_rows, units), half),
            pltpu.HBM((half_rows, width), half),
            pltpu.HBM((n_near, each + SMALL_ROWS, units), half),
        ],
        scratch_shapes=[
            pltpu.VMEM((row_count, units), half),
            pltpu.VMEM((half_rows, units), half),
            pltpu.VMEM((half_rows, width), half),
            pltpu.VMEM((n_near, each + SMALL_ROWS, units), half),
            pltpu.SemaphoreType.DMA((n_near + 1,)),
        ],
        cost_estimate=cost(5 * row_count * width * units, 8 * width * units, row_count * units),
        name="previous_branch",
        compiler_params=pltpu.CompilerParams(vmem_limit_bytes=24 * 2**20),
    )(
        near(x_prev),
        near(plane),
        near(cotangent),
        near(value_prev),
        near(conv_taps),
        near(conv_bias),
    )


def add_halves(keep, weights, from_core, n_x):
    rows, width = from_core.shape
    each = rows // n_x

    def body(keep_ref, w_ref, other_ref, *refs):
        out_refs, blocks_ref, sems = refs[:n_x], refs[n_x], refs[n_x + 1]
        total = lax.dot_general(
            keep_ref[...],
            w_ref[...],
            (((1,), (1,)), ((), ())),
            preferred_element_type=jnp.float32,
        )
        total = (total + other_ref[...].astype(jnp.float32)).astype(jnp.bfloat16)
        moves = []
        for k in range(n_x):
            blocks_ref[k] = total[k * each : (k + 1) * each]
            moves.append(pltpu.make_async_copy(blocks_ref.at[k], out_refs[k], sems.at[k]))
            moves[-1].start()
        for move in moves:
            move.wait()

    return pl.pallas_call(
        body,
        in_specs=[VMEM] * 3,
        out_specs=[HBM] * n_x,
        out_shape=[pltpu.HBM((each, width), jnp.bfloat16)] * n_x,
        scratch_shapes=[
            pltpu.VMEM((n_x, each, width), jnp.bfloat16),
            pltpu.SemaphoreType.DMA((n_x,)),
        ],
        cost_estimate=cost(2 * keep.size * width, 8 * weights.size),
        name="add_halves",
        compiler_params=pltpu.CompilerParams(vmem_limit_bytes=16 * 2**20),
    )(near(keep), near(weights), near(from_core))


def next_branch(x_next, weights, value_next, conv_taps, conv_bias):
    row_count, width = x_next.shape
    units = weights.shape[1]

    def body(x_ref, w_ref, value_ref, taps_ref, bias_ref, out_ref):
        up = jnp.dot(x_ref[...], w_ref[...], preferred_element_type=jnp.float32)
        up = up.astype(jnp.bfloat16).astype(jnp.float32)
        gate = gated(lags_of(up, taps_ref.shape[0]), taps_ref, bias_ref)
        hidden = gate * jax.nn.sigmoid(gate) * value_ref[...].astype(jnp.float32)
        out_ref[...] = hidden.astype(jnp.bfloat16)

    return pl.pallas_call(
        body,
        in_specs=[VMEM] * 5,
        out_shape=jax.ShapeDtypeStruct((row_count, units), jnp.bfloat16),
        cost_estimate=cost(2 * row_count * width * units, 4 * width * units, row_count * units),
        name="next_branch",
        compiler_params=pltpu.CompilerParams(vmem_limit_bytes=24 * 2**20),
    )(near(x_next), near(weights), near(value_next), near(conv_taps), near(conv_bias))


def summed(block):
    return jnp.sum(block.astype(jnp.float32), axis=0)


def small_total(block):
    total = summed(block)
    half = SMALL_ROWS // 2
    rows = lax.broadcasted_iota(jnp.int32, total.shape, 0)
    return jnp.where(rows < half, total + pltpu.roll(total, half, 0), 0.0)


def sum_and_repack(arrived, parts, repeats):
    _, rows, units = arrived.shape
    extra = SMALL_ROWS
    each = (rows - extra) // parts

    def body(in_ref, out_ref, block_ref, sems):
        small = high_and_low(small_total(in_ref[:, rows - extra :]))
        moves = []
        for p in range(parts):
            main = summed(in_ref[:, p * each : (p + 1) * each]).astype(jnp.bfloat16)
            block_ref[p, :each] = main
            block_ref[p, each:] = small
            for r in range(repeats):
                to = r * parts + p
                move = pltpu.make_async_copy(block_ref.at[p], out_ref.at[to], sems.at[to])
                move.start()
                moves.append(move)
        for move in moves:
            move.wait()

    return pl.pallas_call(
        body,
        in_specs=[VMEM],
        out_specs=HBM,
        out_shape=pltpu.HBM((repeats * parts, each + extra, units), jnp.bfloat16),
        scratch_shapes=[
            pltpu.VMEM((parts, each + extra, units), jnp.bfloat16),
            pltpu.SemaphoreType.DMA((repeats * parts,)),
        ],
        cost_estimate=cost(2 * arrived.size, 4 * arrived.size),
        name="sum_and_repack",
        compiler_params=pltpu.CompilerParams(vmem_limit_bytes=24 * 2**20),
    )(near(arrived))


def last_sum(arrived, sum_w, sum_taps, sum_bias):
    rows, _ = sum_w.shape
    tap_count = sum_taps.shape[0]

    def body(in_ref, w_ref, taps_ref, bias_ref, new_w_ref, new_taps_ref, new_bias_ref):
        new_w_ref[...] = w_ref[...] + summed(in_ref[:, :rows])
        small = small_total(in_ref[:, rows:])
        new_taps_ref[...] = taps_ref[...] + small[:tap_count]
        new_bias_ref[...] = bias_ref[...] + small[tap_count]

    return pl.pallas_call(
        body,
        in_specs=[VMEM] * 4,
        out_shape=[
            jax.ShapeDtypeStruct(sum_w.shape, jnp.float32),
            jax.ShapeDtypeStruct(sum_taps.shape, jnp.float32),
            jax.ShapeDtypeStruct(sum_bias.shape, jnp.float32),
        ],
        cost_estimate=cost(2 * arrived.size, 4 * arrived.size),
        name="last_sum",
        compiler_params=pltpu.CompilerParams(vmem_limit_bytes=24 * 2**20),
    )(near(arrived), near(sum_w), near(sum_taps), near(sum_bias))


def per_device(
    x_next,
    value_next,
    x_prev,
    value_prev,
    cotangent,
    w_gate,
    conv_taps,
    conv_bias,
    sum_w,
    sum_taps,
    sum_bias,
):
    row_count, width = x_next.shape
    n_zh, n_x, n_c = (lax.axis_size(a) for a in ("zh", "x", "c"))
    n_far, n_near = lax.axis_size(FAR), lax.axis_size(NEAR)

    plane = copies_to(copies_to(w_gate, FAR, n_far), NEAR, n_near)
    grad_scale = float(row_count * n_zh * n_far * n_near) ** (-0.5)
    grad_value, gathered, keep, to_core, sent = previous_branch(
        x_prev, plane, cotangent, value_prev, conv_taps, conv_bias, grad_scale, n_c
    )
    from_core = send_on(to_core, "c", 1)
    from_near = exchange(sent, NEAR)

    half = add_halves(keep, gathered, from_core, n_x)
    arrived = [half[0]]
    for k in range(1, n_x):
        arrived.append(send_on(half[k], "x", k))
    by_far = sum_and_repack(from_near, n_far, n_zh)
    from_far = exchange(by_far, ("zh", *FAR))

    eighth = sum(block.astype(jnp.float32) for block in arrived).astype(jnp.bfloat16)
    spread = [eighth]
    for k in range(1, n_x):
        spread.append(send_on(eighth, "x", k))
    eighth, x_next = lax.optimization_barrier((eighth, x_next))
    hidden_next = next_branch(x_next, gathered, value_next, conv_taps, conv_bias)
    hidden_next, *spread = lax.optimization_barrier((hidden_next, *spread))
    half = jnp.stack(spread)
    grad_input = put_in_order(half, send_on(half, "c", 1), n_c).reshape(row_count, width)
    from_far, grad_input = lax.optimization_barrier((from_far, grad_input))
    new_w, new_taps, new_bias = last_sum(from_far, sum_w, sum_taps, sum_bias)
    return hidden_next, grad_input, grad_value, new_w, new_taps, new_bias


def solution(mesh):
    n_fs, n_tp = mesh.shape["fs"], mesh.shape["tp"]
    n_y, n_c = 4, 2
    n_z = n_fs // n_y
    fine = Mesh(
        mesh.devices.reshape(mesh.shape["rep"], n_z // 4, 2, 2, n_y, n_tp // n_c, n_c),
        ("zh", *FAR, *NEAR, "x", "c"),
    )
    fs, tp = (*FAR, *NEAR), ("x", "c")
    tokens = ("zh", *fs)
    in_specs = (
        P(tokens, None),
        P(tokens, tp),
        P(tokens, None),
        P(tokens, tp),
        P(tokens, tp),
        P(fs, tp),
        P(None, tp),
        P(tp),
        P(fs, tp),
        P(None, tp),
        P(tp),
    )
    out_specs = (
        P(tokens, tp),
        P(tokens, None),
        P(tokens, tp),
        P(fs, tp),
        P(None, tp),
        P(tp),
    )
    return jax.shard_map(
        per_device, mesh=fine, in_specs=in_specs, out_specs=out_specs, check_vma=False
    )
```
